128 devices in a mesh: rep: 2 (over x_hi), fs: 4 (over x_lo, core), tp: 16 (over z, y).
Axes of the slice: x: 4 (x_hi: 2, x_lo: 2; x = x_hi * 2 + x_lo), y: 4, z: 4, core: 2. Of those that a mesh axis runs over, the one named last changes fastest.
Arguments:
- inputs: bfloat16 [4096, 4096], P(('rep', 'fs', 'tp')), may hold values from -6 to 6
- w_gate: bfloat16 [4096, 11008], P('fs', 'tp'), may hold values from -0.09375 to 0.09375
- w_up: bfloat16 [4096, 11008], P('fs', 'tp'), may hold values from -0.09375 to 0.09375
- w_down: bfloat16 [11008, 4096], P('tp', 'fs'), may hold values from -0.0546875 to 0.0546875
- d_out: bfloat16 [4096, 4096], P(('rep', 'fs', 'tp')), may hold values from -24 to 24
Outputs:
- grad_inputs: bfloat16 [4096, 4096], P(('rep', 'fs', 'tp'))
- grad_gate: float32 [4096, 11008], P('fs', 'tp')
- grad_up: float32 [4096, 11008], P('fs', 'tp')
- grad_down: float32 [11008, 4096], P('tp', 'fs')
The draws below stay inside these ranges and needn't reach their ends.
All inputs are finite; a program needn't handle non-finite values.
Results may differ from the reference program's by a relative error of at most 0.00185.
Values may be sent and summed in bfloat16 or wider, within the bound.
A program may use at most 192 MiB of HBM per device.

```python
import jax
import jax.numpy as jnp
from jax import lax

D = 4096
FF = 11008
TOKENS = 4096


def raised(array, key, source, target, shards_of, factor):
    owner, partner = [(jnp.arange(array.shape[dim]) // (array.shape[dim] // shards_of)).reshape([-1 if axis == dim else 1 for axis in range(array.ndim)]) for dim in (source, target)]
    chosen = jax.random.permutation(key, shards_of)[partner]
    strong = (owner == chosen) | (owner == (partner + shards_of // 2) % shards_of)
    return jnp.where(strong, factor * array, array)


def shard_levels(key, extent, split, least, top_value):
    factor_of, own = 1.0, jax.random.fold_in(key, 6)
    for dim, blocks in split:
        heights = jnp.exp(jax.random.uniform(jax.random.fold_in(own, dim), (blocks,), jnp.float32, least / len(split), top_value / len(split)))
        factor_of = factor_of * jnp.repeat(heights, extent[dim] // blocks).reshape([-1 if axis == dim else 1 for axis in range(len(extent))])
    return factor_of


def centred(stream_key, dims, deviation, reach, pieces=(), kind=jnp.bfloat16):
    array = jax.random.normal(stream_key, dims, jnp.float32) * deviation
    if len(pieces) > 0:
        array = shard_levels(stream_key, dims, pieces, -0.22, 0.18) * array
    return jnp.clip(array, min=-reach, max=reach).astype(kind)


def bell_draw_with(key, extent, scale, reach, pieces, heavy, kind=jnp.bfloat16):
    drawn = scale * jax.random.normal(key, extent, jnp.float32)
    if pieces:
        drawn = drawn * shard_levels(key, extent, pieces, -0.22, 0.18)
    return jnp.clip(raised(drawn, jax.random.fold_in(key, 3), *heavy), -reach, reach).astype(kind)


def setup_inputs(seed: int = 0) -> dict:
    seeds = jax.random.split(jax.random.key(seed), 6)
    inputs = centred(seeds[0], (TOKENS, D), 1.0, 6.0, ((0, 128),))
    w_gate = centred(seeds[1], (D, FF), D ** -0.5, 0.09375, ((0, 4), (1, 16)))
    w_up = centred(seeds[2], (D, FF), D ** -0.5, 0.09375, ((0, 4), (1, 16)))
    w_down = centred(seeds[3], (FF, D), FF ** -0.5, 0.0546875, ((0, 16), (1, 4)))
    d_out = bell_draw_with(seeds[4], (TOKENS, D), 1.0, 24.0, ((0, 128),), (0, 1, 128, 5.5))
    return dict(inputs=inputs, w_gate=w_gate, w_up=w_up, w_down=w_down, d_out=d_out)


def stored(values):
    return lax.optimization_barrier(values.astype(jnp.bfloat16)).astype(jnp.float32)


def reference(inputs, w_gate, w_up, w_down, d_out):
    gate_val = stored(jnp.dot(inputs, w_gate, preferred_element_type=jnp.float32))
    up_val = stored(jnp.dot(inputs, w_up, preferred_element_type=jnp.float32))
    back_val = stored(jnp.dot(d_out, w_down.T, preferred_element_type=jnp.float32))
    sigma = jax.nn.sigmoid(gate_val)
    active = gate_val * sigma
    hidden = (active * up_val).astype(jnp.bfloat16)
    d_gate = (back_val * up_val * sigma * (1.0 + gate_val * (1.0 - sigma))).astype(jnp.bfloat16)
    d_up = (back_val * active).astype(jnp.bfloat16)
    grad_inputs = jnp.dot(d_gate, w_gate.T, preferred_element_type=jnp.float32)
    grad_inputs = grad_inputs + jnp.dot(d_up, w_up.T, preferred_element_type=jnp.float32)
    grad_inputs = grad_inputs.astype(jnp.bfloat16)
    grad_gate = jnp.dot(inputs.T, d_gate, preferred_element_type=jnp.float32)
    grad_up = jnp.dot(inputs.T, d_up, preferred_element_type=jnp.float32)
    grad_down = jnp.dot(hidden.T, d_out, preferred_element_type=jnp.float32)
    return grad_inputs, grad_gate, grad_up, grad_down
```

```python
import jax
import jax.numpy as jnp
from jax import lax
from jax.experimental import pallas as pl
from jax.experimental.pallas import tpu as pltpu
from jax.sharding import PartitionSpec as P

MESH = pl.DeviceIdType.MESH
CUT = 352


def gather_kernel(x_ref, d_ref, wg_ref, wu_ref, wd_ref, xo, do, xp, dp, wgo, wuo, wdo, send, recv, local):
    rep, fs, tp = lax.axis_index("rep"), lax.axis_index("fs"), lax.axis_index("tp")
    core = fs % 2
    xc = rep * 2 + fs // 2
    z, y = tp // 4, tp % 4
    zl, zr, zo = (z + 3) % 4, (z + 1) % 4, (z + 2) % 4
    yl, yr, yo = (y + 3) % 4, (y + 1) % 4, (y + 2) % 4

    def at_x(v):
        return {"rep": v // 2, "fs": (v % 2) * 2 + core}

    xright, xleft = at_x((xc + 1) % 4), at_x((xc + 3) % 4)
    yright, yleft = {"tp": z * 4 + yr}, {"tp": z * 4 + yl}
    zright, zleft = {"tp": zr * 4 + y}, {"tp": zl * 4 + y}
    partner = {"fs": fs + 1 - 2 * core}

    barrier = pltpu.get_barrier_semaphore()
    for dev in (xright, xleft, yright, yleft, zright, zleft, partner):
        pl.semaphore_signal(barrier, inc=1, device_id=dev, device_id_type=MESH)
    pl.semaphore_wait(barrier, 7)

    started = []

    def put(src, dst, dev):
        n = len(started)
        copy = pltpu.make_async_remote_copy(src_ref=src, dst_ref=dst, send_sem=send.at[n], recv_sem=recv.at[n], device_id=dev, device_id_type=MESH)
        copy.start()
        started.append(copy)
        return copy

    def cols(r):
        return pl.ds(1024 * r, 1024)

    head, tail, full = pl.ds(0, CUT), pl.ds(CUT, 688 - CUT), pl.ds(0, 688)
    xa = put(x_ref, xo.at[z, y], yright)
    xb = put(x_ref, xo.at[z, y], yleft)
    da = put(d_ref, do.at[z, y], zright)
    db = put(d_ref, do.at[z, y], zleft)
    w2 = [
        put(wg_ref, wgo.at[full, cols(2)], xright),
        put(wd_ref, wdo.at[full, cols(2)], xleft),
        put(wu_ref.at[head], wuo.at[head, cols(2)], xright),
        put(wu_ref.at[tail], wuo.at[tail, cols(2)], xleft),
    ]
    w1 = [
        put(wg_ref, wgo.at[full, cols(1)], partner),
        put(wu_ref, wuo.at[full, cols(1)], partner),
        put(wd_ref, wdo.at[full, cols(1)], partner),
    ]
    locals_ = []
    for n, (src, dst) in enumerate((
        (x_ref, xo.at[z, y]),
        (d_ref, do.at[z, y]),
        (wg_ref, wgo.at[full, cols(0)]),
        (wu_ref, wuo.at[full, cols(0)]),
        (wd_ref, wdo.at[full, cols(0)]),
    )):
        copy = pltpu.make_async_copy(src, dst, local.at[n])
        copy.start()
        locals_.append(copy)

    lo, hi = pl.ds(0, 16), pl.ds(16, 16)
    xa.wait_recv()
    xc1 = put(xo.at[z, yl, lo], xo.at[z, yl, lo], yright)
    da.wait_recv()
    dc1 = put(do.at[zl, y, lo], do.at[zl, y, lo], zright)
    xb.wait_recv()
    xd1 = put(xo.at[z, yr, hi], xo.at[z, yr, hi], yleft)
    db.wait_recv()
    dd1 = put(do.at[zr, y, hi], do.at[zr, y, hi], zleft)
    locals_[0].wait()
    locals_[1].wait()
    xc1.wait_recv()
    xd1.wait_recv()
    xe = put(xo.at[z], xo.at[z], zright)
    xf = put(xo.at[z], xo.at[z], zleft)
    dc1.wait_recv()
    dd1.wait_recv()
    de = put(do.at[:, y], do.at[:, y], yright)
    df = put(do.at[:, y], do.at[:, y], yleft)

    tails = []

    def hand_x(a, b):
        for j in range(2):
            tails.append(put(xo.at[a, b, :, cols(2 * j + 1)], xp.at[a, b, :, cols(j)], partner))

    def hand_d(a, b):
        for j in range(2):
            tails.append(put(do.at[a, b, :, cols(2 * j + 1)], dp.at[a, b, :, cols(j)], partner))

    every, first, second = pl.ds(0, 4), pl.ds(0, 2), pl.ds(2, 2)
    hand_x(z, every)
    hand_d(every, y)
    xe.wait_recv()
    xg = put(xo.at[zl, first], xo.at[zl, first], zright)
    hand_x(zl, every)
    de.wait_recv()
    dg = put(do.at[first, yl], do.at[first, yl], yright)
    hand_d(every, yl)
    xf.wait_recv()
    xh = put(xo.at[zr, second], xo.at[zr, second], zleft)
    hand_x(zr, every)
    df.wait_recv()
    dh = put(do.at[second, yr], do.at[second, yr], yleft)
    hand_d(every, yr)
    w2[0].wait_recv()
    w3 = [put(wgo.at[full, cols(2)], wgo.at[full, cols(3)], partner)]
    w2[1].wait_recv()
    w3.append(put(wdo.at[full, cols(2)], wdo.at[full, cols(3)], partner))
    xg.wait_recv()
    xh.wait_recv()
    hand_x(zo, every)
    dg.wait_recv()
    dh.wait_recv()
    hand_d(every, yo)
    w2[2].wait_recv()
    w2[3].wait_recv()
    w3.append(put(wuo.at[full, cols(2)], wuo.at[full, cols(3)], partner))
    for copy in w1 + w3 + tails:
        copy.wait_recv()
    for copy in locals_[2:]:
        copy.wait()
    for copy in started:
        copy.wait_send()


COPIES = 42


def gather(x, d, wg, wu, wd):
    b = jnp.bfloat16
    vm = pl.BlockSpec(memory_space=pltpu.VMEM)
    anys = pl.BlockSpec(memory_space=pl.ANY)
    s = jax.ShapeDtypeStruct
    return pl.pallas_call(
        gather_kernel,
        out_shape=[s((4, 4, 32, 4096), b), s((4, 4, 32, 4096), b), s((4, 4, 32, 2048), b), s((4, 4, 32, 2048), b)] + [s((688, 4096), b)] * 3,
        in_specs=[vm] * 5,
        out_specs=[anys] * 7,
        scratch_shapes=[pltpu.SemaphoreType.DMA((COPIES,)), pltpu.SemaphoreType.DMA((COPIES,)), pltpu.SemaphoreType.DMA((5,))],
        compiler_params=pltpu.CompilerParams(collective_id=0, has_side_effects=True),
    )(x, d, wg, wu, wd)


def relative(v, fs):
    v = v.reshape(v.shape[0], 2, 2, 1024)
    v = jnp.where(fs % 2 == 1, v[:, :, ::-1], v)
    v = jnp.where(fs // 2 == 1, v[:, ::-1], v)
    return v.reshape(v.shape[0], 4096)


def stored(values):
    return lax.optimization_barrier(values.astype(jnp.bfloat16)).astype(jnp.float32)


def dot_nt(a, b):
    return lax.dot_general(a, b, (((1,), (1,)), ((), ())), preferred_element_type=jnp.float32)


def dot_tn(a, b):
    return lax.dot_general(a, b, (((0,), (0,)), ((), ())), preferred_element_type=jnp.float32)


def dot_nn(a, b):
    return lax.dot_general(a, b, (((1,), (0,)), ((), ())), preferred_element_type=jnp.float32)


def body(inputs, w_gate, w_up, w_down, d_out):
    fs = lax.axis_index("fs")
    f32, b16 = jnp.float32, jnp.bfloat16
    xo, do, xp, dp, wg, wu, wd = gather(relative(inputs, fs), relative(d_out, fs), w_gate.T, w_up.T, w_down)
    x, d = xo.reshape(512, 4096), do.reshape(512, 4096)
    xp, dp = xp.reshape(512, 2048), dp.reshape(512, 2048)
    gate = stored(dot_nt(x, wg))
    up = stored(dot_nt(x, wu))
    back = stored(dot_nt(d, wd))
    sigma = jax.nn.sigmoid(gate)
    active = gate * sigma
    hidden = (active * up).astype(b16)
    d_gate = (back * up * sigma * (1.0 + gate * (1.0 - sigma))).astype(b16)
    d_up = (back * active).astype(b16)
    other = [(k, k + 1 - 2 * (k % 2)) for k in range(4)]
    hidden_p, d_gate_p, d_up_p = [lax.ppermute(v, "fs", other) for v in (hidden, d_gate, d_up)]

    def ring(v, step):
        return lax.ppermute(v, ("rep", "fs"), [(2 * k + c, 2 * ((k + step) % 4) + c) for k in range(4) for c in range(2)])

    def partial(own, theirs, acts, acts_p, r):
        return dot_tn(own, acts[:, 2048 * r:2048 * r + 1024]) + dot_tn(theirs, acts_p[:, 1024 * r:1024 * r + 1024])

    pg0, pd0, pu0 = partial(d_gate, d_gate_p, x, xp, 0), partial(hidden, hidden_p, d, dp, 0), partial(d_up, d_up_p, x, xp, 0)
    pg1, pd1, pu1 = partial(d_gate, d_gate_p, x, xp, 1), partial(hidden, hidden_p, d, dp, 1), partial(d_up, d_up_p, x, xp, 1)
    sums = []
    for p0, p1 in ((pg0, pg1), (pd0, pd1), (pu0, pu1)):
        q0, q1 = p0.astype(b16), p1.astype(b16)
        a1, b1 = ring(q0[:CUT], 1), ring(q0[CUT:], -1)
        left, right = ring(q1, 1), ring(q1, -1)
        a2, b2 = ring(a1, 1), ring(b1, -1)
        far = jnp.concatenate([a2, b2]).astype(f32)
        sums.append((stored(p0) + far) + (left.astype(f32) + right.astype(f32)))

    dx = dot_nn(d_gate, wg) + dot_nn(d_up, wu)
    dx = lax.psum_scatter(dx, "tp", scatter_dimension=0, tiled=True)
    grad_inputs = relative(dx, fs).astype(b16)
    grad_gate, grad_down, grad_up = sums
    return grad_inputs, grad_gate.T, grad_up.T, grad_down


def solution(mesh):
    tok = P(("rep", "fs", "tp"), None)
    return jax.shard_map(
        body,
        mesh=mesh,
        in_specs=(tok, P("fs", "tp"), P("fs", "tp"), P("tp", "fs"), tok),
        out_specs=(tok, P("fs", "tp"), P("fs", "tp"), P("tp", "fs")),
        check_vma=False,
    )
```

```python
import jax
import jax.numpy as jnp
from jax import lax
from jax.experimental import pallas as pl
from jax.experimental.pallas import tpu as pltpu
from jax.sharding import PartitionSpec as P

MESH = pl.DeviceIdType.MESH
CUT = 352


def gather_kernel(x_ref, d_ref, wg_ref, wu_ref, wd_ref, xo, do, xp, dp, wgo, wuo, wdo, xs, ds, send, recv, local):
    rep, fs, tp = lax.axis_index("rep"), lax.axis_index("fs"), lax.axis_index("tp")
    core = fs % 2
    xc = rep * 2 + fs // 2
    z, y = tp // 4, tp % 4
    zl, zr, zo = (z + 3) % 4, (z + 1) % 4, (z + 2) % 4
    yl, yr, yo = (y + 3) % 4, (y + 1) % 4, (y + 2) % 4

    def at_x(v):
        return {"rep": v // 2, "fs": (v % 2) * 2 + core}

    xright, xleft, xfar = at_x((xc + 1) % 4), at_x((xc + 3) % 4), {"rep": 1 - rep}
    yright, yleft = {"tp": z * 4 + yr}, {"tp": z * 4 + yl}
    zright, zleft = {"tp": zr * 4 + y}, {"tp": zl * 4 + y}
    partner = {"fs": fs + 1 - 2 * core}

    locals_ = []

    def keep(src, dst):
        copy = pltpu.make_async_copy(src, dst, local.at[len(locals_)])
        copy.start()
        locals_.append(copy)

    def cols(r):
        return pl.ds(1024 * r, 1024)

    for q, owner in enumerate((fs, (fs + 2) % 4, fs + 1 - 2 * core, 3 - fs)):
        keep(x_ref.at[:, pl.ds(pl.multiple_of(owner * 1024, 1024), 1024)], xs.at[:, cols(q)])
        keep(d_ref.at[:, pl.ds(pl.multiple_of(owner * 1024, 1024), 1024)], ds.at[:, cols(q)])

    barrier = pltpu.get_barrier_semaphore()
    for dev in (xright, xleft, xfar, yright, yleft, zright, zleft, partner):
        pl.semaphore_signal(barrier, inc=1, device_id=dev, device_id_type=MESH)
    pl.semaphore_wait(barrier, 8)
    for copy in locals_:
        copy.wait()

    started = []

    def put(src, dst, dev):
        n = len(started)
        copy = pltpu.make_async_remote_copy(src_ref=src, dst_ref=dst, send_sem=send.at[n], recv_sem=recv.at[n], device_id=dev, device_id_type=MESH)
        copy.start()
        started.append(copy)
        return copy

    head, tail, full = pl.ds(0, CUT), pl.ds(CUT, 688 - CUT), pl.ds(0, 688)
    lo, hi = pl.ds(0, 16), pl.ds(16, 16)
    every, first, second = pl.ds(0, 4), pl.ds(0, 2), pl.ds(2, 2)
    gathered = []

    def first_axis(k, xsrc, dsrc):
        return [
            put(xsrc, xo.at[k, z, y], yright),
            put(dsrc, do.at[k, z, y], zright),
            put(xsrc, xo.at[k, z, y], yleft),
            put(dsrc, do.at[k, z, y], zleft),
        ]

    def first_axis_far(k, c):
        c[0].wait_recv()
        a = put(xo.at[k, z, yl, lo], xo.at[k, z, yl, lo], yright)
        c[1].wait_recv()
        b = put(do.at[k, zl, y, lo], do.at[k, zl, y, lo], zright)
        c[2].wait_recv()
        e = put(xo.at[k, z, yr, hi], xo.at[k, z, yr, hi], yleft)
        c[3].wait_recv()
        f = put(do.at[k, zr, y, hi], do.at[k, zr, y, hi], zleft)
        return [a, e, b, f]

    def hand_x(k, a):
        gathered.append(put(xo.at[k, a, :, :, pl.ds(2048, 2048)], xp.at[k, a], partner))

    def hand_d(k, a):
        gathered.append(put(do.at[k, :, a, :, pl.ds(2048, 2048)], dp.at[k, :, a], partner))

    def second_axis(k, c):
        c[0].wait_recv()
        c[1].wait_recv()
        a = put(xo.at[k, z], xo.at[k, z], zright)
        b = put(xo.at[k, z], xo.at[k, z], zleft)
        c[2].wait_recv()
        c[3].wait_recv()
        e = put(do.at[k, :, y], do.at[k, :, y], yright)
        f = put(do.at[k, :, y], do.at[k, :, y], yleft)
        hand_x(k, z)
        hand_d(k, y)
        return [a, e, b, f]

    def second_axis_far(k, c):
        c[0].wait_recv()
        a = put(xo.at[k, zl, first], xo.at[k, zl, first], zright)
        hand_x(k, zl)
        c[1].wait_recv()
        b = put(do.at[k, first, yl], do.at[k, first, yl], yright)
        hand_d(k, yl)
        c[2].wait_recv()
        e = put(xo.at[k, zr, second], xo.at[k, zr, second], zleft)
        hand_x(k, zr)
        c[3].wait_recv()
        f = put(do.at[k, second, yr], do.at[k, second, yr], yleft)
        hand_d(k, yr)
        return [a, e, b, f]

    def finish(k, c):
        c[0].wait_recv()
        c[1].wait_recv()
        hand_x(k, zo)
        c[2].wait_recv()
        c[3].wait_recv()
        hand_d(k, yo)

    far = [put(xs, xo.at[1, z, y], xfar), put(ds, do.at[1, z, y], xfar)]
    own1 = first_axis(0, xs, ds)
    w2 = [
        put(wg_ref, wgo.at[full, cols(1)], xright),
        put(wd_ref, wdo.at[full, cols(1)], xleft),
        put(wu_ref.at[head], wuo.at[head, cols(1)], xright),
        put(wu_ref.at[tail], wuo.at[tail, cols(1)], xleft),
    ]
    w1 = [
        put(wg_ref, wgo.at[full, cols(2)], partner),
        put(wu_ref, wuo.at[full, cols(2)], partner),
        put(wd_ref, wdo.at[full, cols(2)], partner),
    ]
    keep(xs, xo.at[0, z, y])
    keep(ds, do.at[0, z, y])
    keep(wg_ref, wgo.at[full, cols(0)])
    keep(wu_ref, wuo.at[full, cols(0)])
    keep(wd_ref, wdo.at[full, cols(0)])

    own2 = first_axis_far(0, own1)
    far[0].wait_recv()
    far[1].wait_recv()
    far1 = first_axis(1, xo.at[1, z, y], do.at[1, z, y])
    locals_[8].wait()
    locals_[9].wait()
    own3 = second_axis(0, own2)
    far2 = first_axis_far(1, far1)
    far3 = second_axis(1, far2)
    own4 = second_axis_far(0, own3)
    w2[0].wait_recv()
    w3 = [put(wgo.at[full, cols(1)], wgo.at[full, cols(3)], partner)]
    w2[1].wait_recv()
    w3.append(put(wdo.at[full, cols(1)], wdo.at[full, cols(3)], partner))
    w2[2].wait_recv()
    w2[3].wait_recv()
    w3.append(put(wuo.at[full, cols(1)], wuo.at[full, cols(3)], partner))
    finish(0, own4)
    far4 = second_axis_far(1, far3)
    finish(1, far4)
    for copy in w1 + w3 + gathered:
        copy.wait_recv()
    for copy in locals_[10:]:
        copy.wait()
    for copy in started:
        copy.wait_send()


COPIES = 60


def gather(x, d, wg, wu, wd):
    b = jnp.bfloat16
    vm = pl.BlockSpec(memory_space=pltpu.VMEM)
    anys = pl.BlockSpec(memory_space=pl.ANY)
    s = jax.ShapeDtypeStruct
    return pl.pallas_call(
        gather_kernel,
        out_shape=[s((2, 4, 4, 32, 4096), b)] * 2 + [s((2, 4, 4, 32, 2048), b)] * 2 + [s((688, 4096), b)] * 3,
        in_specs=[anys] * 2 + [vm] * 3,
        out_specs=[anys] * 7,
        scratch_shapes=[
            pltpu.VMEM((32, 4096), b),
            pltpu.VMEM((32, 4096), b),
            pltpu.SemaphoreType.DMA((COPIES,)),
            pltpu.SemaphoreType.DMA((COPIES,)),
            pltpu.SemaphoreType.DMA((13,)),
        ],
        compiler_params=pltpu.CompilerParams(collective_id=0, has_side_effects=True),
    )(x, d, wg, wu, wd)


def stored(values):
    return lax.optimization_barrier(values.astype(jnp.bfloat16)).astype(jnp.float32)


def dot_nt(a, b):
    return lax.dot_general(a, b, (((1,), (1,)), ((), ())), preferred_element_type=jnp.float32)


def dot_tn(a, b):
    return lax.dot_general(a, b, (((0,), (0,)), ((), ())), preferred_element_type=jnp.float32)


def dot_nn(a, b):
    return lax.dot_general(a, b, (((1,), (0,)), ((), ())), preferred_element_type=jnp.float32)


def body(inputs, w_gate, w_up, w_down, d_out):
    fs = lax.axis_index("fs")
    f32, b16 = jnp.float32, jnp.bfloat16
    xo, do, xp, dp, wg, wu, wd = gather(inputs, d_out, w_gate.T, w_up.T, w_down)
    x, d = xo.reshape(1024, 4096), do.reshape(1024, 4096)
    xp, dp = xp.reshape(1024, 2048), dp.reshape(1024, 2048)
    gate = stored(dot_nt(x, wg))
    up = stored(dot_nt(x, wu))
    back = stored(dot_nt(d, wd))
    sigma = jax.nn.sigmoid(gate)
    active = gate * sigma
    hidden = (active * up).astype(b16)
    d_gate = (back * up * sigma * (1.0 + gate * (1.0 - sigma))).astype(b16)
    d_up = (back * active).astype(b16)
    other = [(k, k + 1 - 2 * (k % 2)) for k in range(4)]
    hidden_p, d_gate_p, d_up_p = [lax.ppermute(v, "fs", other) for v in (hidden, d_gate, d_up)]

    def ring(v, step):
        return lax.ppermute(v, ("rep", "fs"), [(2 * k + c, 2 * ((k + step) % 4) + c) for k in range(4) for c in range(2)])

    def partial(own, theirs, acts, acts_p, r):
        return dot_tn(own, acts[:, 1024 * r:1024 * r + 1024]) + dot_tn(theirs, acts_p[:, 1024 * r:1024 * r + 1024])

    dx = dot_nn(d_gate[:512], wg) + dot_nn(d_up[:512], wu)
    dx = lax.psum_scatter(dx, "tp", scatter_dimension=0, tiled=True)
    terms = ((d_gate, d_gate_p, x, xp), (d_up, d_up_p, x, xp), (hidden, hidden_p, d, dp))
    arrived = []
    for t in terms:
        p = partial(*t, 1).astype(b16)
        arrived.append((ring(p[:CUT], 1), ring(p[CUT:], -1)))
    sums = [partial(*t, 0) + jnp.concatenate(a).astype(f32) for t, a in zip(terms, arrived)]
    dx = dx.reshape(32, 2, 2, 1024)
    dx = jnp.swapaxes(dx, 1, 2)
    dx = jnp.where(fs % 2 == 1, dx[:, :, ::-1], dx)
    dx = jnp.where(fs // 2 == 1, dx[:, ::-1], dx)
    grad_inputs = dx.reshape(32, 4096).astype(b16)
    return grad_inputs, sums[0].T, sums[1].T, sums[2]


def solution(mesh):
    tok = P(("rep", "fs", "tp"), None)
    return jax.shard_map(
        body,
        mesh=mesh,
        in_specs=(tok, P("fs", "tp"), P("fs", "tp"), P("tp", "fs"), tok),
        out_specs=(tok, P("fs", "tp"), P("fs", "tp"), P("tp", "fs")),
        check_vma=False,
    )
```

```python
import jax
import jax.numpy as jnp
from jax import lax
from jax.experimental import pallas as pl
from jax.experimental.pallas import tpu as pltpu
from jax.sharding import PartitionSpec as P

MESH = pl.DeviceIdType.MESH
CUT = 352


def dot_nt(a, b):
    return lax.dot_general(a, b, (((1,), (1,)), ((), ())), preferred_element_type=jnp.float32)


def dot_tn(a, b):
    return lax.dot_general(a, b, (((0,), (0,)), ((), ())), preferred_element_type=jnp.float32)


def kernel(x_ref, d_ref, wg_ref, wu_ref, wd_ref, gi, og, ou, od, xo0, xo1, do0, do1, xp, dp, xs, ds, wv, xv, dv, pre, hv, h1, hp0, hp1, dxv, r1, r2, r3, t1, t2, t3, wr, p0, send, recv, local):
    xo, do = (xo0, xo1), (do0, do1)
    rep, fs, tp = lax.axis_index("rep"), lax.axis_index("fs"), lax.axis_index("tp")
    core = fs % 2
    xc = rep * 2 + fs // 2
    z, y = tp // 4, tp % 4

    def at_x(v):
        return {"rep": v // 2, "fs": (v % 2) * 2 + core}

    xright, xleft, xfar = at_x((xc + 1) % 4), at_x((xc + 3) % 4), {"rep": 1 - rep}
    yright, yleft = {"tp": z * 4 + (y + 1) % 4}, {"tp": z * 4 + (y + 3) % 4}
    zright, zleft = {"tp": ((z + 1) % 4) * 4 + y}, {"tp": ((z + 3) % 4) * 4 + y}
    partner = {"fs": fs + 1 - 2 * core}
    owners = (fs, (fs + 2) % 4, fs + 1 - 2 * core, 3 - fs)
    counts = [0]

    def keep(src, dst):
        copy = pltpu.make_async_copy(src, dst, local.at[counts[0]])
        counts[0] += 1
        copy.start()
        return copy

    started = []

    def put(src, dst, dev):
        n = len(started)
        copy = pltpu.make_async_remote_copy(src_ref=src, dst_ref=dst, send_sem=send.at[n], recv_sem=recv.at[n], device_id=dev, device_id_type=MESH)
        copy.start()
        started.append(copy)
        return copy

    def block(r):
        return pl.ds(1024 * r, 1024)

    ready = []
    for q, owner in enumerate(owners):
        span = pl.ds(pl.multiple_of(owner * 1024, 1024), 1024)
        ready += [keep(x_ref.at[:, span], xs.at[:, block(q)]), keep(d_ref.at[:, span], ds.at[:, block(q)])]
    for m, ref in enumerate((wg_ref, wu_ref, wd_ref)):
        ready.append(keep(ref, wv.at[m, :, block(0)]))

    barrier = pltpu.get_barrier_semaphore()
    for dev in (xright, xleft, xfar, yright, yleft, zright, zleft, partner):
        pl.semaphore_signal(barrier, inc=1, device_id=dev, device_id_type=MESH)
    pl.semaphore_wait(barrier, 8)
    for copy in ready:
        copy.wait()

    head, tail = pl.ds(0, CUT), pl.ds(CUT, 688 - CUT)
    lo, hi = pl.ds(0, 16), pl.ds(16, 16)
    first, second = pl.ds(0, 2), pl.ds(2, 2)
    gathered = []

    def first_axis(k, xsrc, dsrc):
        return [
            put(xsrc, xo[k].at[0, 1], yright),
            put(dsrc, do[k].at[1, 0], zright),
            put(xsrc, xo[k].at[0, 2], yleft),
            put(dsrc, do[k].at[2, 0], zleft),
        ]

    def first_axis_far(k, c):
        c[0].wait_recv()
        a = put(xo[k].at[0, 1, lo], xo[k].at[0, 3, lo], yright)
        c[1].wait_recv()
        b = put(do[k].at[1, 0, lo], do[k].at[3, 0, lo], zright)
        c[2].wait_recv()
        e = put(xo[k].at[0, 2, hi], xo[k].at[0, 3, hi], yleft)
        c[3].wait_recv()
        f = put(do[k].at[2, 0, hi], do[k].at[3, 0, hi], zleft)
        return [a, e, b, f]

    def hand_x(k, a):
        gathered.append(put(xo[k].at[a, :, :, pl.ds(2048, 2048)], xp.at[k, a], partner))

    def hand_d(k, a):
        gathered.append(put(do[k].at[:, a, :, pl.ds(2048, 2048)], dp.at[k, :, a], partner))

    def second_axis(k, c):
        c[0].wait_recv()
        c[1].wait_recv()
        a = put(xo[k].at[0], xo[k].at[1], zright)
        b = put(xo[k].at[0], xo[k].at[2], zleft)
        c[2].wait_recv()
        c[3].wait_recv()
        e = put(do[k].at[:, 0], do[k].at[:, 1], yright)
        f = put(do[k].at[:, 0], do[k].at[:, 2], yleft)
        hand_x(k, 0)
        hand_d(k, 0)
        return [a, e, b, f]

    def second_axis_far(k, c):
        c[0].wait_recv()
        a = put(xo[k].at[1, first], xo[k].at[3, first], zright)
        hand_x(k, 1)
        c[1].wait_recv()
        b = put(do[k].at[first, 1], do[k].at[first, 3], yright)
        hand_d(k, 1)
        c[2].wait_recv()
        e = put(xo[k].at[2, second], xo[k].at[3, second], zleft)
        hand_x(k, 2)
        c[3].wait_recv()
        f = put(do[k].at[second, 2], do[k].at[second, 3], yleft)
        hand_d(k, 2)
        return [a, e, b, f]

    def finish(k, c):
        c[0].wait_recv()
        c[1].wait_recv()
        hand_x(k, 3)
        c[2].wait_recv()
        c[3].wait_recv()
        hand_d(k, 3)

    far = [put(xs, xo[1].at[0, 0], xfar), put(ds, do[1].at[0, 0], xfar)]
    own1 = first_axis(0, xs, ds)
    w2 = [
        put(wv.at[0, :, block(0)], wv.at[0, :, block(1)], xright),
        put(wv.at[2, :, block(0)], wv.at[2, :, block(1)], xleft),
        put(wv.at[1, head, block(0)], wv.at[1, head, block(1)], xright),
        put(wv.at[1, tail, block(0)], wv.at[1, tail, block(1)], xleft),
    ]
    w1 = [put(wv.at[m, :, block(0)], wv.at[m, :, block(2)], partner) for m in range(3)]
    own0 = [keep(xs, xo[0].at[0, 0]), keep(ds, do[0].at[0, 0])]

    own2 = first_axis_far(0, own1)
    far[0].wait_recv()
    far[1].wait_recv()
    far1 = first_axis(1, xo[1].at[0, 0], do[1].at[0, 0])
    for copy in own0:
        copy.wait()
    own3 = second_axis(0, own2)
    far2 = first_axis_far(1, far1)
    w2[0].wait_recv()
    w3 = [put(wv.at[0, :, block(1)], wv.at[0, :, block(3)], partner)]
    w2[1].wait_recv()
    w3.append(put(wv.at[2, :, block(1)], wv.at[2, :, block(3)], partner))
    own4 = second_axis_far(0, own3)
    far3 = second_axis(1, far2)
    w2[2].wait_recv()
    w2[3].wait_recv()
    w3.append(put(wv.at[1, :, block(1)], wv.at[1, :, block(3)], partner))
    finish(0, own4)

    whole = [keep(xo0, xv), keep(do0, dv)]
    for copy in w1 + w3:
        copy.wait_recv()
    for copy in whole:
        copy.wait()

    def forward(m, acts, n):
        rows = acts[pl.ds(n * 2, 2)].reshape(256, 4096)
        pre[m, :, pl.ds(pl.multiple_of(n * 256, 256), 256)] = dot_nt(wv[m], rows).astype(jnp.bfloat16)

    def pointwise(h):
        @pl.loop(0, 43)
        def _(n):
            rows = pl.ds(pl.multiple_of(n * 16, 16), 16)
            gate, up, back = [pre[m, rows, :].astype(jnp.float32) for m in range(3)]
            sigma = 1.0 / (1.0 + jnp.exp(-gate))
            active = gate * sigma
            h[0, rows, :] = (back * up * sigma * (1.0 + gate * (1.0 - sigma))).astype(jnp.bfloat16)
            h[1, rows, :] = (back * active).astype(jnp.bfloat16)
            h[2, rows, :] = (active * up).astype(jnp.bfloat16)

    for m, acts in enumerate((xv, xv, dv)):
        @pl.loop(0, 2)
        def _(n):
            forward(m, acts, n)

    pointwise(hv)
    swap0 = put(hv, hp0, partner)
    far4 = second_axis_far(1, far3)
    whole = [keep(xo1.at[first], xv.at[first]), keep(xo1.at[2], xv.at[2]), keep(do1.at[:, pl.ds(0, 3)], dv.at[:, pl.ds(0, 3)])]

    @pl.loop(0, 8)
    def _(n):
        span = pl.ds(pl.multiple_of(n * 512, 512), 512)
        total = dot_tn(hv[0], wv[0, :, span]) + dot_tn(hv[1], wv[1, :, span])
        dxv[:, :, :, span] = total.reshape(4, 4, 32, 512)

    def slab(c, k, h):
        span = pl.ds(2048 * c + 1024 * h, 1024)
        return dxv.at[:, k, :, span] if c == 0 else dxv.at[k, :, :, span]

    def part(c, k, h):
        return r2.at[c, h, k]

    ways = ((yleft, yright), (zleft, zright))

    def send_raw(view, way, c, a1, a3):
        return [
            put(view(c, 3, 0), a1.at[c, 0], way[1]),
            put(view(c, 3, 1), a1.at[c, 1], way[0]),
            put(view(c, 2, 1), a3.at[c, 1], way[1]),
            put(view(c, 1, 0), a3.at[c, 0], way[0]),
        ]

    def send_summed(view, way, c, a1, a2, copies):
        copies[0].wait_recv()
        a1[c, 0] += view(c, 2, 0)[...]
        one = put(a1.at[c, 0], a2.at[c, 0], way[1])
        copies[1].wait_recv()
        a1[c, 1] += view(c, 1, 1)[...]
        return [one, put(a1.at[c, 1], a2.at[c, 1], way[0])]

    sums1 = [send_raw(slab, ways[c], c, r1, r3) for c in range(2)]
    whole[0].wait()
    forward(0, xv, 0)
    forward(1, xv, 0)
    finish(1, far4)
    last_x, last_d = keep(xo1.at[3], xv.at[3]), keep(do1.at[:, 3], dv.at[:, 3])
    whole[1].wait()
    last_x.wait()
    forward(0, xv, 1)
    forward(1, xv, 1)
    for copy in gathered:
        copy.wait_recv()

    def load(k, tokens, theirs, r):
        return [
            keep(source, (xv, dv)[k].at[:, :, :, block(q)])
            for q, source in enumerate((tokens[0].at[:, :, :, block(r)], tokens[1].at[:, :, :, block(r)], theirs.at[0, :, :, :, block(r)], theirs.at[1, :, :, :, block(r)]))
        ]

    loads_x = load(0, xo, xp, 1)
    whole[2].wait()
    last_d.wait()

    @pl.loop(0, 2)
    def _(n):
        forward(2, dv, n)

    loads_d = load(1, do, dp, 1)
    pointwise(h1)
    swaps = [put(h1.at[m], hp1.at[m], partner) for m in range(3)]
    sums2 = [send_summed(slab, ways[c], c, r1, r2, sums1[c]) for c in range(2)]

    def product(m, acts, n):
        total = None
        for q, h in enumerate((hv, h1, hp0, hp1)):
            span = pl.ds(pl.multiple_of(q * 1024 + n * 256, 256), 256)
            term = jnp.dot(h[m], acts[:, :, :, span].reshape(512, 256), preferred_element_type=jnp.float32)
            total = term if total is None else total + term
        return total

    crossing = []

    def outgoing(m, acts):
        for half in range(2):
            @pl.loop(2 * half, 2 * half + 2)
            def _(n):
                wv[m, :, pl.ds(pl.multiple_of(n * 256, 256), 256)] = product(m, acts, n).astype(jnp.bfloat16)

            span = pl.ds(512 * half, 512)
            crossing.append(put(wv.at[m, head, span], wr.at[m, head, span], xright))
            crossing.append(put(wv.at[m, tail, span], wr.at[m, tail, span], xleft))

    def kept(m, acts, slot):
        @pl.loop(0, 4)
        def _(n):
            p0[slot, :, pl.ds(pl.multiple_of(n * 256, 256), 256)] = product(m, acts, n)

    def close(m, slot, ref):
        for copy in crossing[4 * m:4 * m + 4]:
            copy.wait_recv()

        @pl.loop(0, 4)
        def _(n):
            span = pl.ds(pl.multiple_of(n * 256, 256), 256)
            p0[slot, :, span] += wr[m, :, span].astype(jnp.float32)

        return keep(p0.at[slot], ref)

    for copy in loads_x:
        copy.wait()
    swap0.wait_recv()
    swaps[0].wait_recv()
    for copy in w1 + w2:
        copy.wait_send()
    outgoing(0, xv)
    swaps[1].wait_recv()
    outgoing(1, xv)
    loads_x = load(0, xo, xp, 0)
    for copy in loads_d:
        copy.wait()
    swaps[2].wait_recv()
    outgoing(2, dv)
    loads_d = load(1, do, dp, 0)
    sums3 = []
    for c in range(2):
        sums1[c][3].wait_recv()
        sums2[c][0].wait_recv()
        r2[c, 0] += slab(c, 0, 0)[...] + r3[c, 0]
        sums1[c][2].wait_recv()
        sums2[c][1].wait_recv()
        r2[c, 1] += slab(c, 0, 1)[...] + r3[c, 1]
        sums3.append(send_raw(part, ways[1 - c], c, t1, t3))
    for copy in loads_x:
        copy.wait()
    kept(0, xv, 0)
    kept(1, xv, 1)
    sums4 = [send_summed(part, ways[1 - c], c, t1, t2, sums3[c]) for c in range(2)]
    out0 = close(0, 0, og)
    for c in range(2):
        sums3[c][3].wait_recv()
        sums4[c][0].wait_recv()
        sums3[c][2].wait_recv()
        sums4[c][1].wait_recv()
        for h in range(2):
            total = part(c, 0, h)[...] + (t2[c, h] + t3[c, h])
            gi[:, pl.ds(pl.multiple_of(owners[2 * c + h] * 1024, 1024), 1024)] = total.astype(jnp.bfloat16)
    for copy in loads_d:
        copy.wait()
    out0.wait()
    kept(2, dv, 0)
    out1 = close(1, 1, ou)
    out2 = close(2, 0, od)
    out1.wait()
    out2.wait()
    for copy in started:
        if not any(copy is done for done in w1 + w2):
            copy.wait_send()


SENDS, KEPT = 100, 39


def body(inputs, w_gate, w_up, w_down, d_out):
    b, f = jnp.bfloat16, jnp.float32
    vm = pl.BlockSpec(memory_space=pltpu.VMEM)
    anys = pl.BlockSpec(memory_space=pl.ANY)
    s = jax.ShapeDtypeStruct
    outs = pl.pallas_call(
        kernel,
        out_shape=[s((32, 4096), b)] + [s((688, 1024), f)] * 3 + [s((4, 4, 32, 4096), b)] * 4 + [s((2, 4, 4, 32, 2048), b)] * 2,
        in_specs=[anys] * 5,
        out_specs=[vm] + [anys] * 9,
        scratch_shapes=[pltpu.VMEM((32, 4096), b)] * 2
        + [pltpu.VMEM((3, 688, 4096), b)]
        + [pltpu.VMEM((4, 4, 32, 4096), b)] * 2
        + [pltpu.VMEM((3, 688, 512), b)] * 5
        + [pltpu.VMEM((4, 4, 32, 4096), f)]
        + [pltpu.VMEM((2, 2, 4, 32, 1024), f)] * 3
        + [pltpu.VMEM((2, 2, 32, 1024), f)] * 3
        + [pltpu.VMEM((3, 688, 1024), b)]
        + [pltpu.VMEM((2, 688, 1024), f)]
        + [pltpu.SemaphoreType.DMA((SENDS,)), pltpu.SemaphoreType.DMA((SENDS,)), pltpu.SemaphoreType.DMA((KEPT,))],
        compiler_params=pltpu.CompilerParams(collective_id=0, has_side_effects=True, vmem_limit_bytes=67043328),
    )(inputs, d_out, w_gate.T, w_up.T, w_down)
    return outs[0], outs[1].T, outs[2].T, outs[3]


def solution(mesh):
    tok = P(("rep", "fs", "tp"), None)
    return jax.shard_map(
        body,
        mesh=mesh,
        in_specs=(tok, P("fs", "tp"), P("fs", "tp"), P("tp", "fs"), tok),
        out_specs=(tok, P("fs", "tp"), P("fs", "tp"), P("tp", "fs")),
        check_vma=False,
    )
```

```python
import jax
import jax.numpy as jnp
from jax import lax
from jax.experimental import pallas as pl
from jax.experimental.pallas import tpu as pltpu
from jax.sharding import PartitionSpec as P

MESH = pl.DeviceIdType.MESH
CUT = 352


def dot_nt(a, b):
    return lax.dot_general(a, b, (((1,), (1,)), ((), ())), preferred_element_type=jnp.float32)


def dot_tn(a, b):
    return lax.dot_general(a, b, (((0,), (0,)), ((), ())), preferred_element_type=jnp.float32)


def kernel(x_ref, d_ref, wg_ref, wu_ref, wd_ref, gi, og, ou, od, xo0, xo1, do0, do1, xp, dp, rx, rd, xs, ds, fx, fd, wv, xv, dv, back_ref, hv, h1, hp0, hp1, dxv, r1, r2, r3, t1, t2, t3, wr, send, recv, local):
    xo, do = (xo0, xo1), (do0, do1)
    rep, fs, tp = lax.axis_index("rep"), lax.axis_index("fs"), lax.axis_index("tp")
    core = fs % 2
    xc = rep * 2 + fs // 2
    z, y = tp // 4, tp % 4

    def at_x(v):
        return {"rep": v // 2, "fs": (v % 2) * 2 + core}

    xright, xleft, xfar = at_x((xc + 1) % 4), at_x((xc + 3) % 4), {"rep": 1 - rep}
    yright, yleft = {"tp": z * 4 + (y + 1) % 4}, {"tp": z * 4 + (y + 3) % 4}
    zright, zleft = {"tp": ((z + 1) % 4) * 4 + y}, {"tp": ((z + 3) % 4) * 4 + y}
    partner = {"fs": fs + 1 - 2 * core}
    owners = (fs, (fs + 2) % 4, fs + 1 - 2 * core, 3 - fs)
    counts = [0]

    def keep(src, dst):
        copy = pltpu.make_async_copy(src, dst, local.at[counts[0]])
        counts[0] += 1
        copy.start()
        return copy

    started = []

    def put(src, dst, dev):
        n = len(started)
        copy = pltpu.make_async_remote_copy(src_ref=src, dst_ref=dst, send_sem=send.at[n], recv_sem=recv.at[n], device_id=dev, device_id_type=MESH)
        copy.start()
        started.append(copy)
        return copy

    def block(r):
        return pl.ds(1024 * r, 1024)

    ready = []
    for q, owner in enumerate(owners):
        span = pl.ds(pl.multiple_of(owner * 1024, 1024), 1024)
        ready += [keep(x_ref.at[:, span], xs.at[:, block(q)]), keep(d_ref.at[:, span], ds.at[:, block(q)])]
    for m, ref in enumerate((wg_ref, wu_ref, wd_ref)):
        ready.append(keep(ref, wv.at[m, :, block(0)]))

    barrier = pltpu.get_barrier_semaphore()
    for dev in (xright, xleft, xfar, yright, yleft, zright, zleft, partner):
        pl.semaphore_signal(barrier, inc=1, device_id=dev, device_id_type=MESH)
    pl.semaphore_wait(barrier, 8)
    for copy in ready[:8]:
        copy.wait()

    head, tail = pl.ds(0, CUT), pl.ds(CUT, 688 - CUT)
    lo, hi = pl.ds(0, 16), pl.ds(16, 16)
    first, second = pl.ds(0, 2), pl.ds(2, 2)
    gathered = []

    def first_axis(k, xsrc, dsrc):
        return [
            put(xsrc, xo[k].at[0, 1], yright),
            put(dsrc, do[k].at[1, 0], zright),
            put(xsrc, xo[k].at[0, 2], yleft),
            put(dsrc, do[k].at[2, 0], zleft),
        ]

    def first_axis_far(k, c):
        c[0].wait_recv()
        a = put(xo[k].at[0, 1, lo], xo[k].at[0, 3, lo], yright)
        c[1].wait_recv()
        b = put(do[k].at[1, 0, lo], do[k].at[3, 0, lo], zright)
        c[2].wait_recv()
        e = put(xo[k].at[0, 2, hi], xo[k].at[0, 3, hi], yleft)
        c[3].wait_recv()
        f = put(do[k].at[2, 0, hi], do[k].at[3, 0, hi], zleft)
        return [a, e, b, f]

    def hand_x(k, a):
        gathered.append(put(xo[k].at[a, :, :, pl.ds(2048, 2048)], xp.at[k, a], partner))

    def hand_d(k, a):
        gathered.append(put(do[k].at[:, a, :, pl.ds(2048, 2048)], dp.at[k, :, a], partner))

    def second_axis(k, c):
        c[0].wait_recv()
        c[1].wait_recv()
        x = [put(xo[k].at[0, half], xo[k].at[slot, half], dev) for half, slot, dev in ((first, 1, zright), (second, 2, zleft), (second, 1, zright), (first, 2, zleft))]
        c[2].wait_recv()
        c[3].wait_recv()
        d = [put(do[k].at[half, 0], do[k].at[half, slot], dev) for half, slot, dev in ((first, 1, yright), (second, 2, yleft), (second, 1, yright), (first, 2, yleft))]
        hand_x(k, 0)
        hand_d(k, 0)
        return x, d

    def second_axis_far(k, c):
        first, second = ((pl.ds(0, 2), pl.ds(2, 2)), (pl.ds(0, 1), pl.ds(3, 1)))[k]
        x, d = c
        x[0].wait_recv()
        a = put(xo[k].at[1, first], xo[k].at[3, first], zright)
        d[0].wait_recv()
        b = put(do[k].at[first, 1], do[k].at[first, 3], yright)
        x[1].wait_recv()
        e = put(xo[k].at[2, second], xo[k].at[3, second], zleft)
        d[1].wait_recv()
        f = put(do[k].at[second, 2], do[k].at[second, 3], yleft)
        return [a, e, b, f]

    def rest(k, c):
        x, d = c
        for n in range(2):
            x[2 + n].wait_recv()
            hand_x(k, 1 + n)
            d[2 + n].wait_recv()
            hand_d(k, 1 + n)

    def finish(k, c):
        c[0].wait_recv()
        c[1].wait_recv()
        hand_x(k, 3)
        c[2].wait_recv()
        c[3].wait_recv()
        hand_d(k, 3)

    hops = [put(xs, fx, xright), put(ds, fd, xleft)]
    own1 = first_axis(0, xs, ds)
    own0 = [keep(xs, xo[0].at[0, 0]), keep(ds, do[0].at[0, 0])]

    for copy in ready[8:]:
        copy.wait()
    w1 = [put(wv.at[m, :, block(0)], wv.at[m, :, block(2)], partner) for m in range(3)]
    hops[0].wait_recv()
    far = [put(fx, xo[1].at[0, 0], xright)]
    hops[1].wait_recv()
    far.append(put(fd, do[1].at[0, 0], xleft))
    w2 = [
        put(wv.at[0, :, block(0)], wv.at[0, :, block(1)], xright),
        put(wv.at[2, :, block(0)], wv.at[2, :, block(1)], xleft),
        put(wv.at[1, head, block(0)], wv.at[1, head, block(1)], xright),
        put(wv.at[1, tail, block(0)], wv.at[1, tail, block(1)], xleft),
    ]
    own2 = first_axis_far(0, own1)
    far[0].wait_recv()
    far[1].wait_recv()
    far1 = first_axis(1, xo[1].at[0, 0], do[1].at[0, 0])
    for copy in own0:
        copy.wait()
    own3 = second_axis(0, own2)
    far2 = first_axis_far(1, far1)
    own4 = second_axis_far(0, own3)
    w2[0].wait_recv()
    w3 = [put(wv.at[0, :, block(1)], wv.at[0, :, block(3)], partner)]
    w2[1].wait_recv()
    w3.append(put(wv.at[2, :, block(1)], wv.at[2, :, block(3)], partner))
    rest(0, own3)
    far3 = second_axis(1, far2)
    w2[2].wait_recv()
    w2[3].wait_recv()
    w3.append(put(wv.at[1, :, block(1)], wv.at[1, :, block(3)], partner))
    finish(0, own4)
    middle = pl.ds(1, 2)
    helped = [put(xo0.at[3, middle], rx, xright), put(do0.at[middle, 3], rd, xleft)]

    whole = [keep(xo0, xv), keep(do0, dv)]
    for copy in w1 + w3:
        copy.wait_recv()
    for copy in whole:
        copy.wait()

    def forward(ref, m, acts, n):
        rows = acts[pl.ds(n * 2, 2)].reshape(256, 4096)
        ref[:, pl.ds(pl.multiple_of(n * 256, 256), 256)] = dot_nt(wv[m], rows).astype(jnp.bfloat16)

    def pointwise(h, inner, outer):
        @pl.loop(0, 43)
        def _(n):
            rows = pl.ds(pl.multiple_of(n * 16, 16), 16)
            gate = h[0, rows, :].astype(jnp.float32)
            up = h[1, rows, :].astype(jnp.float32)
            sigma = 1.0 / (1.0 + jnp.exp(-gate))
            active = gate * sigma
            if inner:
                h[2, rows, :] = (active * up).astype(jnp.bfloat16)
            if outer:
                back = back_ref[rows, :].astype(jnp.float32)
                h[0, rows, :] = (back * up * sigma * (1.0 + gate * (1.0 - sigma))).astype(jnp.bfloat16)
                h[1, rows, :] = (back * active).astype(jnp.bfloat16)

    for m, acts in enumerate((xv, xv, dv)):
        @pl.loop(0, 2)
        def _(n):
            forward((hv.at[0], hv.at[1], back_ref)[m], m, acts, n)

    helped[0].wait_recv()
    relay = [put(rx, xo1.at[3, middle], xright)]
    helped[1].wait_recv()
    relay.append(put(rd, do1.at[middle, 3], xleft))
    far4 = second_axis_far(1, far3)
    pointwise(hv, True, True)
    swap0 = put(hv, hp0, partner)
    rest(1, far3)
    whole = [keep(xo1.at[first], xv.at[first]), keep(xo1.at[2], xv.at[2]), keep(do1.at[:, pl.ds(0, 3)], dv.at[:, pl.ds(0, 3)])]

    @pl.loop(0, 8)
    def _(n):
        span = pl.ds(pl.multiple_of(n * 512, 512), 512)
        total = dot_tn(hv[0], wv[0, :, span]) + dot_tn(hv[1], wv[1, :, span])
        dxv[:, :, :, span] = total.reshape(4, 4, 32, 512)

    def slab(c, k, h):
        span = pl.ds(2048 * c + 1024 * h, 1024)
        return dxv.at[:, k, :, span] if c == 0 else dxv.at[k, :, :, span]

    def part(c, k, h):
        return r2.at[c, h, k]

    ways = ((yleft, yright), (zleft, zright))

    def send_raw(view, way, c, a1, a3):
        return [
            put(view(c, 3, 0), a1.at[c, 0], way[1]),
            put(view(c, 3, 1), a1.at[c, 1], way[0]),
            put(view(c, 2, 1), a3.at[c, 1], way[1]),
            put(view(c, 1, 0), a3.at[c, 0], way[0]),
        ]

    def send_summed(view, way, c, a1, a2, copies):
        copies[0].wait_recv()
        a1[c, 0] += view(c, 2, 0)[...]
        one = put(a1.at[c, 0], a2.at[c, 0], way[1])
        copies[1].wait_recv()
        a1[c, 1] += view(c, 1, 1)[...]
        return [one, put(a1.at[c, 1], a2.at[c, 1], way[0])]

    sums1 = [send_raw(slab, ways[c], c, r1, r3) for c in range(2)]
    whole[0].wait()
    forward(h1.at[0], 0, xv, 0)
    forward(h1.at[1], 1, xv, 0)
    for copy in relay:
        copy.wait_recv()
    finish(1, far4)
    last_x, last_d = keep(xo1.at[3], xv.at[3]), keep(do1.at[:, 3], dv.at[:, 3])
    whole[1].wait()
    last_x.wait()
    forward(h1.at[0], 0, xv, 1)
    forward(h1.at[1], 1, xv, 1)
    pointwise(h1, True, False)
    swaps = {2: put(h1.at[2], hp1.at[2], partner)}
    for copy in gathered:
        copy.wait_recv()

    def load(k, tokens, theirs, r):
        return [
            keep(source, (xv, dv)[k].at[:, :, :, block(q)])
            for q, source in enumerate((tokens[0].at[:, :, :, block(r)], tokens[1].at[:, :, :, block(r)], theirs.at[0, :, :, :, block(r)], theirs.at[1, :, :, :, block(r)]))
        ]

    loads_x = load(0, xo, xp, 1)
    whole[2].wait()
    last_d.wait()

    @pl.loop(0, 2)
    def _(n):
        forward(back_ref, 2, dv, n)

    loads_d = load(1, do, dp, 1)
    pointwise(h1, False, True)
    for m in range(2):
        swaps[m] = put(h1.at[m], hp1.at[m], partner)

    def product(m, acts, n):
        total = None
        for q, h in enumerate((hv, h1, hp0, hp1)):
            span = pl.ds(pl.multiple_of(q * 1024 + n * 256, 256), 256)
            term = jnp.dot(h[m], acts[:, :, :, span].reshape(512, 256), preferred_element_type=jnp.float32)
            total = term if total is None else total + term
        return total

    crossing = {}

    def outgoing(m, acts):
        for half in range(2):
            @pl.loop(2 * half, 2 * half + 2)
            def _(n):
                wv[m, :, pl.ds(pl.multiple_of(n * 256, 256), 256)] = product(m, acts, n).astype(jnp.bfloat16)

            span = pl.ds(512 * half, 512)
            crossing[m, half] = [put(wv.at[m, head, span], wr.at[m, head, span], xright), put(wv.at[m, tail, span], wr.at[m, tail, span], xleft)]

    def kept(m, acts, ref):
        @pl.loop(0, 4)
        def _(n):
            ref[:, pl.ds(pl.multiple_of(n * 256, 256), 256)] = product(m, acts, n)

    def close(m, ref):
        for half in range(2):
            for copy in crossing[m, half]:
                copy.wait_recv()

            @pl.loop(2 * half, 2 * half + 2)
            def _(n):
                span = pl.ds(pl.multiple_of(n * 256, 256), 256)
                ref[:, span] += wr[m, :, span].astype(jnp.float32)

    for copy in loads_d:
        copy.wait()
    swap0.wait_recv()
    swaps[2].wait_recv()
    for copy in w1 + w2:
        copy.wait_send()
    outgoing(2, dv)
    loads_d = load(1, do, dp, 0)
    sums2 = [send_summed(slab, ways[c], c, r1, r2, sums1[c]) for c in range(2)]
    for copy in loads_x:
        copy.wait()
    swaps[0].wait_recv()
    outgoing(0, xv)
    swaps[1].wait_recv()
    outgoing(1, xv)
    loads_x = load(0, xo, xp, 0)
    sums3 = []
    for c in range(2):
        sums1[c][3].wait_recv()
        sums2[c][0].wait_recv()
        r2[c, 0] += slab(c, 0, 0)[...] + r3[c, 0]
        sums1[c][2].wait_recv()
        sums2[c][1].wait_recv()
        r2[c, 1] += slab(c, 0, 1)[...] + r3[c, 1]
        sums3.append(send_raw(part, ways[1 - c], c, t1, t3))
    for copy in loads_d:
        copy.wait()
    kept(2, dv, od)
    for copy in loads_x:
        copy.wait()
    kept(0, xv, og)
    kept(1, xv, ou)
    sums4 = [send_summed(part, ways[1 - c], c, t1, t2, sums3[c]) for c in range(2)]
    close(2, od)
    for c in range(2):
        sums3[c][3].wait_recv()
        sums4[c][0].wait_recv()
        sums3[c][2].wait_recv()
        sums4[c][1].wait_recv()
        for h in range(2):
            total = part(c, 0, h)[...] + (t2[c, h] + t3[c, h])
            gi[:, pl.ds(pl.multiple_of(owners[2 * c + h] * 1024, 1024), 1024)] = total.astype(jnp.bfloat16)
    close(0, og)
    close(1, ou)
    for copy in started:
        if not any(copy is done for done in w1 + w2):
            copy.wait_send()


SENDS, KEPT, LIMIT = 120, 42, 58000000


def body(inputs, w_gate, w_up, w_down, d_out):
    b, f = jnp.bfloat16, jnp.float32
    vm = pl.BlockSpec(memory_space=pltpu.VMEM)
    anys = pl.BlockSpec(memory_space=pl.ANY)
    s = jax.ShapeDtypeStruct
    outs = pl.pallas_call(
        kernel,
        out_shape=[pltpu.VMEM((32, 4096), b)] + [pltpu.VMEM((688, 1024), f)] * 3 + [s((4, 4, 32, 4096), b)] * 4 + [s((2, 4, 4, 32, 2048), b)] * 2 + [s((2, 32, 4096), b)] * 2,
        in_specs=[anys] * 5,
        out_specs=[vm] * 4 + [anys] * 8,
        scratch_shapes=[pltpu.VMEM((32, 4096), b)] * 4
        + [pltpu.VMEM((3, 688, 4096), b)]
        + [pltpu.VMEM((4, 4, 32, 4096), b)] * 2
        + [pltpu.VMEM((688, 512), b)]
        + [pltpu.VMEM((3, 688, 512), b)] * 4
        + [pltpu.VMEM((4, 4, 32, 4096), f)]
        + [pltpu.VMEM((2, 2, 4, 32, 1024), f)] * 3
        + [pltpu.VMEM((2, 2, 32, 1024), f)] * 3
        + [pltpu.VMEM((3, 688, 1024), b)]
        + [pltpu.SemaphoreType.DMA((SENDS,)), pltpu.SemaphoreType.DMA((SENDS,)), pltpu.SemaphoreType.DMA((KEPT,))],
        compiler_params=pltpu.CompilerParams(collective_id=0, has_side_effects=True, vmem_limit_bytes=LIMIT),
    )(inputs, d_out, w_gate.T, w_up.T, w_down)
    return outs[0], outs[1].T, outs[2].T, outs[3]


def solution(mesh):
    tok = P(("rep", "fs", "tp"), None)
    return jax.shard_map(
        body,
        mesh=mesh,
        in_specs=(tok, P("fs", "tp"), P("fs", "tp"), P("tp", "fs"), tok),
        out_specs=(tok, P("fs", "tp"), P("fs", "tp"), P("tp", "fs")),
        check_vma=False,
    )
```

```python
import jax
import jax.numpy as jnp
from jax import lax
from jax.experimental import pallas as pl
from jax.experimental.pallas import tpu as pltpu
from jax.sharding import PartitionSpec as P

MESH = pl.DeviceIdType.MESH
CUT = 352


def dot_nt(a, b):
    return lax.dot_general(a, b, (((1,), (1,)), ((), ())), preferred_element_type=jnp.float32)


def dot_tn(a, b):
    return lax.dot_general(a, b, (((0,), (0,)), ((), ())), preferred_element_type=jnp.float32)


def kernel(x_ref, d_ref, wg_ref, wu_ref, wd_ref, gi, og, ou, od, xo0, xo1, do0, do1, xp, dp, xs, ds, fx, fd, wv, xv, dv, back_ref, hv, h1, hp0, hp1, dxv, r1, r2, r3, t1, t2, t3, wr, send, recv, local):
    xo, do = (xv, xo1), (dv, do1)
    rep, fs, tp = lax.axis_index("rep"), lax.axis_index("fs"), lax.axis_index("tp")
    core = fs % 2
    xc = rep * 2 + fs // 2
    z, y = tp // 4, tp % 4

    def at_x(v):
        return {"rep": v // 2, "fs": (v % 2) * 2 + core}

    xright, xleft = at_x((xc + 1) % 4), at_x((xc + 3) % 4)
    yright, yleft = {"tp": z * 4 + (y + 1) % 4}, {"tp": z * 4 + (y + 3) % 4}
    zright, zleft = {"tp": ((z + 1) % 4) * 4 + y}, {"tp": ((z + 3) % 4) * 4 + y}
    partner = {"fs": fs + 1 - 2 * core}
    owners = (fs, (fs + 2) % 4, fs + 1 - 2 * core, 3 - fs)
    counts = [0]

    def keep(src, dst):
        copy = pltpu.make_async_copy(src, dst, local.at[counts[0]])
        counts[0] += 1
        copy.start()
        return copy

    started = []

    def put(src, dst, dev):
        n = len(started)
        copy = pltpu.make_async_remote_copy(src_ref=src, dst_ref=dst, send_sem=send.at[n], recv_sem=recv.at[n], device_id=dev, device_id_type=MESH)
        copy.start()
        started.append(copy)
        return copy

    def block(r):
        return pl.ds(1024 * r, 1024)

    ready = []
    for q, owner in enumerate(owners):
        span = pl.ds(pl.multiple_of(owner * 1024, 1024), 1024)
        ready += [keep(x_ref.at[:, span], xs.at[:, block(q)]), keep(d_ref.at[:, span], ds.at[:, block(q)])]
    for m, ref in enumerate((wg_ref, wu_ref, wd_ref)):
        ready.append(keep(ref, wv.at[m, :, block(0)]))

    barrier = pltpu.get_barrier_semaphore()
    for dev in (xright, xleft, yright, yleft, zright, zleft, partner):
        pl.semaphore_signal(barrier, inc=1, device_id=dev, device_id_type=MESH)
    pl.semaphore_wait(barrier, 7)
    for copy in ready[:8]:
        copy.wait()

    head, tail = pl.ds(0, CUT), pl.ds(CUT, 688 - CUT)
    lo, hi = pl.ds(0, 16), pl.ds(16, 16)
    first, second = pl.ds(0, 2), pl.ds(2, 2)
    gathered = []

    def first_axis(k, xsrc, dsrc):
        return [
            put(xsrc, xo[k].at[0, 1], yright),
            put(dsrc, do[k].at[1, 0], zright),
            put(xsrc, xo[k].at[0, 2], yleft),
            put(dsrc, do[k].at[2, 0], zleft),
        ]

    def first_axis_far(k, c):
        c[0].wait_recv()
        a = put(xo[k].at[0, 1, lo], xo[k].at[0, 3, lo], yright)
        c[1].wait_recv()
        b = put(do[k].at[1, 0, lo], do[k].at[3, 0, lo], zright)
        c[2].wait_recv()
        e = put(xo[k].at[0, 2, hi], xo[k].at[0, 3, hi], yleft)
        c[3].wait_recv()
        f = put(do[k].at[2, 0, hi], do[k].at[3, 0, hi], zleft)
        return [a, e, b, f]

    def hand_x(k, a):
        gathered.append(put(xo[k].at[a, :, :, pl.ds(2048, 2048)], xp.at[k, a], partner))

    def hand_d(k, a):
        gathered.append(put(do[k].at[:, a, :, pl.ds(2048, 2048)], dp.at[k, :, a], partner))

    def second_axis(k, c):
        c[0].wait_recv()
        c[1].wait_recv()
        x = [put(xo[k].at[0, half], xo[k].at[slot, half], dev) for half, slot, dev in ((first, 1, zright), (second, 2, zleft), (second, 1, zright), (first, 2, zleft))]
        c[2].wait_recv()
        c[3].wait_recv()
        d = [put(do[k].at[half, 0], do[k].at[half, slot], dev) for half, slot, dev in ((first, 1, yright), (second, 2, yleft), (second, 1, yright), (first, 2, yleft))]
        hand_x(k, 0)
        hand_d(k, 0)
        return x, d

    def second_axis_far(k, c):
        first, second = ((pl.ds(0, 2), pl.ds(2, 2)), (pl.ds(0, 2), pl.ds(2, 2)))[k]
        x, d = c
        x[0].wait_recv()
        a = put(xo[k].at[1, first], xo[k].at[3, first], zright)
        d[0].wait_recv()
        b = put(do[k].at[first, 1], do[k].at[first, 3], yright)
        x[1].wait_recv()
        e = put(xo[k].at[2, second], xo[k].at[3, second], zleft)
        d[1].wait_recv()
        f = put(do[k].at[second, 2], do[k].at[second, 3], yleft)
        return [a, e, b, f]

    def rest(k, c):
        x, d = c
        for n in range(2):
            x[2 + n].wait_recv()
            hand_x(k, 1 + n)
            d[2 + n].wait_recv()
            hand_d(k, 1 + n)

    def finish(k, c):
        c[0].wait_recv()
        c[1].wait_recv()
        hand_x(k, 3)
        c[2].wait_recv()
        c[3].wait_recv()
        hand_d(k, 3)

    hops = [put(xs, fx, xright), put(ds, fd, xleft)]
    own1 = first_axis(0, xs, ds)
    own0 = [keep(xs, xo[0].at[0, 0]), keep(ds, do[0].at[0, 0])]

    for copy in ready[8:]:
        copy.wait()
    w1 = [put(wv.at[m, :, block(0)], wv.at[m, :, block(2)], partner) for m in range(3)]
    hops[0].wait_recv()
    far = [put(fx, xo[1].at[0, 0], xright)]
    hops[1].wait_recv()
    far.append(put(fd, do[1].at[0, 0], xleft))
    w2 = [
        put(wv.at[0, :, block(0)], wv.at[0, :, block(1)], xright),
        put(wv.at[2, :, block(0)], wv.at[2, :, block(1)], xleft),
        put(wv.at[1, head, block(0)], wv.at[1, head, block(1)], xright),
        put(wv.at[1, tail, block(0)], wv.at[1, tail, block(1)], xleft),
    ]
    own2 = first_axis_far(0, own1)
    for copy in own0:
        copy.wait()
    own3 = second_axis(0, own2)
    far[0].wait_recv()
    far[1].wait_recv()
    far1 = first_axis(1, xo[1].at[0, 0], do[1].at[0, 0])
    far2 = first_axis_far(1, far1)
    own4 = second_axis_far(0, own3)
    w2[0].wait_recv()
    w3 = [put(wv.at[0, :, block(1)], wv.at[0, :, block(3)], partner)]
    w2[1].wait_recv()
    w3.append(put(wv.at[2, :, block(1)], wv.at[2, :, block(3)], partner))
    rest(0, own3)
    far3 = second_axis(1, far2)
    w2[2].wait_recv()
    w2[3].wait_recv()
    w3.append(put(wv.at[1, :, block(1)], wv.at[1, :, block(3)], partner))
    finish(0, own4)

    early = len(started)
    sent = list(started)
    whole = [keep(xv, xo0), keep(dv, do0)]
    for copy in w1 + w3:
        copy.wait_recv()

    def forward(ref, m, acts, n):
        rows = acts[pl.ds(n * 2, 2)].reshape(256, 4096)
        ref[:, pl.ds(pl.multiple_of(n * 256, 256), 256)] = dot_nt(wv[m], rows).astype(jnp.bfloat16)

    def pointwise(h, inner, outer):
        @pl.loop(0, 43)
        def _(n):
            rows = pl.ds(pl.multiple_of(n * 16, 16), 16)
            gate = h[0, rows, :].astype(jnp.float32)
            up = h[1, rows, :].astype(jnp.float32)
            sigma = 1.0 / (1.0 + jnp.exp(-gate))
            active = gate * sigma
            if inner:
                h[2, rows, :] = (active * up).astype(jnp.bfloat16)
            if outer:
                back = back_ref[rows, :].astype(jnp.float32)
                h[0, rows, :] = (back * up * sigma * (1.0 + gate * (1.0 - sigma))).astype(jnp.bfloat16)
                h[1, rows, :] = (back * active).astype(jnp.bfloat16)

    for m, acts in enumerate((xv, xv, dv)):
        @pl.loop(0, 2)
        def _(n):
            forward((hv.at[0], hv.at[1], back_ref)[m], m, acts, n)

    far4 = second_axis_far(1, far3)
    pointwise(hv, True, True)
    swap0 = put(hv, hp0, partner)
    rest(1, far3)
    for copy in whole:
        copy.wait()
    for copy in sent:
        copy.wait_send()
    whole = [keep(xo1.at[first], xv.at[first]), keep(xo1.at[2], xv.at[2]), keep(do1.at[:, pl.ds(0, 3)], dv.at[:, pl.ds(0, 3)])]

    @pl.loop(0, 8)
    def _(n):
        span = pl.ds(pl.multiple_of(n * 512, 512), 512)
        total = dot_tn(hv[0], wv[0, :, span]) + dot_tn(hv[1], wv[1, :, span])
        dxv[:, :, :, span] = total.reshape(4, 4, 32, 512)

    def slab(c, k, h):
        span = pl.ds(2048 * c + 1024 * h, 1024)
        return dxv.at[:, k, :, span] if c == 0 else dxv.at[k, :, :, span]

    def part(c, k, h):
        return r2.at[c, h, k]

    ways = ((yleft, yright), (zleft, zright))

    def send_raw(view, way, c, a1, a3):
        return [
            put(view(c, 3, 0), a1.at[c, 0], way[1]),
            put(view(c, 3, 1), a1.at[c, 1], way[0]),
            put(view(c, 2, 1), a3.at[c, 1], way[1]),
            put(view(c, 1, 0), a3.at[c, 0], way[0]),
        ]

    def send_summed(view, way, c, a1, a2, copies):
        copies[0].wait_recv()
        a1[c, 0] += view(c, 2, 0)[...]
        one = put(a1.at[c, 0], a2.at[c, 0], way[1])
        copies[1].wait_recv()
        a1[c, 1] += view(c, 1, 1)[...]
        return [one, put(a1.at[c, 1], a2.at[c, 1], way[0])]

    sums1 = [send_raw(slab, ways[c], c, r1, r3) for c in range(2)]
    whole[0].wait()
    forward(h1.at[0], 0, xv, 0)
    forward(h1.at[1], 1, xv, 0)
    finish(1, far4)
    last_x, last_d = keep(xo1.at[3], xv.at[3]), keep(do1.at[:, 3], dv.at[:, 3])
    whole[1].wait()
    last_x.wait()
    forward(h1.at[0], 0, xv, 1)
    forward(h1.at[1], 1, xv, 1)
    pointwise(h1, True, False)
    swaps = {2: put(h1.at[2], hp1.at[2], partner)}
    for copy in gathered:
        copy.wait_recv()

    def load(k, tokens, theirs, r):
        return [
            keep(source, (xv, dv)[k].at[:, :, :, block(q)])
            for q, source in enumerate((tokens[0].at[:, :, :, block(r)], tokens[1].at[:, :, :, block(r)], theirs.at[0, :, :, :, block(r)], theirs.at[1, :, :, :, block(r)]))
        ]

    loads_x = load(0, (xo0, xo1), xp, 1)
    whole[2].wait()
    last_d.wait()

    @pl.loop(0, 2)
    def _(n):
        forward(back_ref, 2, dv, n)

    loads_d = load(1, (do0, do1), dp, 1)
    pointwise(h1, False, True)
    for m in range(2):
        swaps[m] = put(h1.at[m], hp1.at[m], partner)

    def product(m, acts, n):
        total = None
        for q, h in enumerate((hv, h1, hp0, hp1)):
            span = pl.ds(pl.multiple_of(q * 1024 + n * 256, 256), 256)
            term = jnp.dot(h[m], acts[:, :, :, span].reshape(512, 256), preferred_element_type=jnp.float32)
            total = term if total is None else total + term
        return total

    crossing = {}

    def outgoing(m, acts):
        for half in range(2):
            @pl.loop(2 * half, 2 * half + 2)
            def _(n):
                wv[m, :, pl.ds(pl.multiple_of(n * 256, 256), 256)] = product(m, acts, n).astype(jnp.bfloat16)

            span = pl.ds(512 * half, 512)
            crossing[m, half] = [put(wv.at[m, head, span], wr.at[m, head, span], xright), put(wv.at[m, tail, span], wr.at[m, tail, span], xleft)]

    def kept(m, acts, ref):
        @pl.loop(0, 4)
        def _(n):
            ref[:, pl.ds(pl.multiple_of(n * 256, 256), 256)] = product(m, acts, n)

    def close(m, ref):
        for half in range(2):
            for copy in crossing[m, half]:
                copy.wait_recv()

            @pl.loop(2 * half, 2 * half + 2)
            def _(n):
                span = pl.ds(pl.multiple_of(n * 256, 256), 256)
                ref[:, span] += wr[m, :, span].astype(jnp.float32)

    for copy in loads_d:
        copy.wait()
    swap0.wait_recv()
    swaps[2].wait_recv()
    outgoing(2, dv)
    loads_d = load(1, (do0, do1), dp, 0)
    sums2 = [send_summed(slab, ways[c], c, r1, r2, sums1[c]) for c in range(2)]
    for copy in loads_x:
        copy.wait()
    swaps[0].wait_recv()
    outgoing(0, xv)
    swaps[1].wait_recv()
    outgoing(1, xv)
    loads_x = load(0, (xo0, xo1), xp, 0)
    sums3 = []
    for c in range(2):
        sums1[c][3].wait_recv()
        sums2[c][0].wait_recv()
        r2[c, 0] += slab(c, 0, 0)[...] + r3[c, 0]
        sums1[c][2].wait_recv()
        sums2[c][1].wait_recv()
        r2[c, 1] += slab(c, 0, 1)[...] + r3[c, 1]
        sums3.append(send_raw(part, ways[1 - c], c, t1, t3))
    for copy in loads_d:
        copy.wait()
    kept(2, dv, od)
    for copy in loads_x:
        copy.wait()
    kept(0, xv, og)
    kept(1, xv, ou)
    sums4 = [send_summed(part, ways[1 - c], c, t1, t2, sums3[c]) for c in range(2)]
    close(2, od)
    for c in range(2):
        sums3[c][3].wait_recv()
        sums4[c][0].wait_recv()
        sums3[c][2].wait_recv()
        sums4[c][1].wait_recv()
        for h in range(2):
            total = part(c, 0, h)[...] + (t2[c, h] + t3[c, h])
            gi[:, pl.ds(pl.multiple_of(owners[2 * c + h] * 1024, 1024), 1024)] = total.astype(jnp.bfloat16)
    close(0, og)
    close(1, ou)
    for copy in started[early:]:
        copy.wait_send()


SENDS, KEPT, LIMIT = 120, 42, 58000000


def body(inputs, w_gate, w_up, w_down, d_out):
    b, f = jnp.bfloat16, jnp.float32
    vm = pl.BlockSpec(memory_space=pltpu.VMEM)
    anys = pl.BlockSpec(memory_space=pl.ANY)
    s = jax.ShapeDtypeStruct
    outs = pl.pallas_call(
        kernel,
        out_shape=[pltpu.VMEM((32, 4096), b)] + [pltpu.VMEM((688, 1024), f)] * 3 + [s((4, 4, 32, 4096), b)] * 4 + [s((2, 4, 4, 32, 2048), b)] * 2,
        in_specs=[anys] * 5,
        out_specs=[vm] * 4 + [anys] * 6,
        scratch_shapes=[pltpu.VMEM((32, 4096), b)] * 4
        + [pltpu.VMEM((3, 688, 4096), b)]
        + [pltpu.VMEM((4, 4, 32, 4096), b)] * 2
        + [pltpu.VMEM((688, 512), b)]
        + [pltpu.VMEM((3, 688, 512), b)] * 4
        + [pltpu.VMEM((4, 4, 32, 4096), f)]
        + [pltpu.VMEM((2, 2, 4, 32, 1024), f)] * 3
        + [pltpu.VMEM((2, 2, 32, 1024), f)] * 3
        + [pltpu.VMEM((3, 688, 1024), b)]
        + [pltpu.SemaphoreType.DMA((SENDS,)), pltpu.SemaphoreType.DMA((SENDS,)), pltpu.SemaphoreType.DMA((KEPT,))],
        compiler_params=pltpu.CompilerParams(collective_id=0, has_side_effects=True, vmem_limit_bytes=LIMIT),
    )(inputs, d_out, w_gate.T, w_up.T, w_down)
    return outs[0], outs[1].T, outs[2].T, outs[3]


def solution(mesh):
    tok = P(("rep", "fs", "tp"), None)
    return jax.shard_map(
        body,
        mesh=mesh,
        in_specs=(tok, P("fs", "tp"), P("fs", "tp"), P("tp", "fs"), tok),
        out_specs=(tok, P("fs", "tp"), P("fs", "tp"), P("tp", "fs")),
        check_vma=False,
    )
```

```python
import jax
import jax.numpy as jnp
from jax import lax
from jax.experimental import pallas as pl
from jax.experimental.pallas import tpu as pltpu
from jax.sharding import PartitionSpec as P

MESH = pl.DeviceIdType.MESH
CUT = 352


def dot_nt(a, b):
    return lax.dot_general(a, b, (((1,), (1,)), ((), ())), preferred_element_type=jnp.float32)


def dot_tn(a, b):
    return lax.dot_general(a, b, (((0,), (0,)), ((), ())), preferred_element_type=jnp.float32)


def kernel(x_ref, d_ref, wg_ref, wu_ref, wd_ref, gi, og, ou, od, xo0, xo1, do0, do1, xp, dp, xs, ds, fx, fd, wv, xv, dv, back_ref, hv, h1, hp0, hp1, dxv, r1, r2, r3, t1, t2, t3, wr, send, recv, local):
    xo, do = (xv, xo1), (dv, do1)
    rep, fs, tp = lax.axis_index("rep"), lax.axis_index("fs"), lax.axis_index("tp")
    core = fs % 2
    xc = rep * 2 + fs // 2
    z, y = tp // 4, tp % 4

    def at_x(v):
        return {"rep": v // 2, "fs": (v % 2) * 2 + core}

    xright, xleft = at_x((xc + 1) % 4), at_x((xc + 3) % 4)
    yright, yleft = {"tp": z * 4 + (y + 1) % 4}, {"tp": z * 4 + (y + 3) % 4}
    zright, zleft = {"tp": ((z + 1) % 4) * 4 + y}, {"tp": ((z + 3) % 4) * 4 + y}
    partner = {"fs": fs + 1 - 2 * core}
    owners = (fs, (fs + 2) % 4, fs + 1 - 2 * core, 3 - fs)
    counts = [0]

    def keep(src, dst):
        copy = pltpu.make_async_copy(src, dst, local.at[counts[0]])
        counts[0] += 1
        copy.start()
        return copy

    started = []

    def put(src, dst, dev):
        n = len(started)
        copy = pltpu.make_async_remote_copy(src_ref=src, dst_ref=dst, send_sem=send.at[n], recv_sem=recv.at[n], device_id=dev, device_id_type=MESH)
        copy.start()
        started.append(copy)
        return copy

    def block(r):
        return pl.ds(1024 * r, 1024)

    ready = []
    for q, owner in enumerate(owners):
        span = pl.ds(pl.multiple_of(owner * 1024, 1024), 1024)
        ready += [keep(x_ref.at[:, span], xs.at[:, block(q)]), keep(d_ref.at[:, span], ds.at[:, block(q)])]
    for m, ref in enumerate((wg_ref, wu_ref, wd_ref)):
        ready.append(keep(ref, wv.at[m, :, block(0)]))

    barrier = pltpu.get_barrier_semaphore()
    for dev in (xright, xleft, yright, yleft, zright, zleft, partner):
        pl.semaphore_signal(barrier, inc=1, device_id=dev, device_id_type=MESH)
    pl.semaphore_wait(barrier, 7)
    for copy in ready[:8]:
        copy.wait()

    head, tail = pl.ds(0, CUT), pl.ds(CUT, 688 - CUT)
    lo, hi = pl.ds(0, 16), pl.ds(16, 16)
    first, second = pl.ds(0, 2), pl.ds(2, 2)
    gathered = []

    def first_axis(k, xsrc, dsrc):
        return [
            put(xsrc, xo[k].at[0, 1], yright),
            put(dsrc, do[k].at[1, 0], zright),
            put(xsrc, xo[k].at[0, 2], yleft),
            put(dsrc, do[k].at[2, 0], zleft),
        ]

    def first_axis_far(k, c):
        c[0].wait_recv()
        a = put(xo[k].at[0, 1, lo], xo[k].at[0, 3, lo], yright)
        c[1].wait_recv()
        b = put(do[k].at[1, 0, lo], do[k].at[3, 0, lo], zright)
        c[2].wait_recv()
        e = put(xo[k].at[0, 2, hi], xo[k].at[0, 3, hi], yleft)
        c[3].wait_recv()
        f = put(do[k].at[2, 0, hi], do[k].at[3, 0, hi], zleft)
        return [a, e, b, f]

    def hand_x(k, a):
        gathered.append(put(xo[k].at[a, :, :, pl.ds(2048, 2048)], xp.at[k, a], partner))

    def hand_d(k, a):
        gathered.append(put(do[k].at[:, a, :, pl.ds(2048, 2048)], dp.at[k, :, a], partner))

    def second_axis(k, c):
        c[0].wait_recv()
        c[1].wait_recv()
        x = [put(xo[k].at[0, half], xo[k].at[slot, half], dev) for half, slot, dev in ((first, 1, zright), (second, 2, zleft), (second, 1, zright), (first, 2, zleft))]
        c[2].wait_recv()
        c[3].wait_recv()
        d = [put(do[k].at[half, 0], do[k].at[half, slot], dev) for half, slot, dev in ((first, 1, yright), (second, 2, yleft), (second, 1, yright), (first, 2, yleft))]
        hand_x(k, 0)
        hand_d(k, 0)
        return x, d

    def second_axis_far(k, c):
        first, second = ((pl.ds(0, 2), pl.ds(2, 2)), (pl.ds(0, 2), pl.ds(2, 2)))[k]
        x, d = c
        x[0].wait_recv()
        a = put(xo[k].at[1, first], xo[k].at[3, first], zright)
        d[0].wait_recv()
        b = put(do[k].at[first, 1], do[k].at[first, 3], yright)
        x[1].wait_recv()
        e = put(xo[k].at[2, second], xo[k].at[3, second], zleft)
        d[1].wait_recv()
        f = put(do[k].at[second, 2], do[k].at[second, 3], yleft)
        return [a, e, b, f]

    def rest(k, c):
        x, d = c
        for n in range(2):
            x[2 + n].wait_recv()
            hand_x(k, 1 + n)
            d[2 + n].wait_recv()
            hand_d(k, 1 + n)

    def finish(k, c):
        c[0].wait_recv()
        c[1].wait_recv()
        hand_x(k, 3)
        c[2].wait_recv()
        c[3].wait_recv()
        hand_d(k, 3)

    hops = [put(xs, fx, xright), put(ds, fd, xleft)]
    own1 = first_axis(0, xs, ds)
    own0 = [keep(xs, xo[0].at[0, 0]), keep(ds, do[0].at[0, 0])]

    for copy in ready[8:]:
        copy.wait()
    w1 = [put(wv.at[m, :, block(0)], wv.at[m, :, block(2)], partner) for m in range(3)]
    hops[0].wait_recv()
    far = [put(fx, xo[1].at[0, 0], xright)]
    hops[1].wait_recv()
    far.append(put(fd, do[1].at[0, 0], xleft))
    w2 = [
        put(wv.at[0, :, block(0)], wv.at[0, :, block(1)], xright),
        put(wv.at[2, :, block(0)], wv.at[2, :, block(1)], xleft),
        put(wv.at[1, head, block(0)], wv.at[1, head, block(1)], xright),
        put(wv.at[1, tail, block(0)], wv.at[1, tail, block(1)], xleft),
    ]
    own2 = first_axis_far(0, own1)
    for copy in own0:
        copy.wait()
    own3 = second_axis(0, own2)
    far[0].wait_recv()
    far[1].wait_recv()
    far1 = first_axis(1, xo[1].at[0, 0], do[1].at[0, 0])
    far2 = first_axis_far(1, far1)
    own4 = second_axis_far(0, own3)
    w2[0].wait_recv()
    w3 = [put(wv.at[0, :, block(1)], wv.at[0, :, block(3)], partner)]
    w2[1].wait_recv()
    w3.append(put(wv.at[2, :, block(1)], wv.at[2, :, block(3)], partner))
    rest(0, own3)
    far3 = second_axis(1, far2)
    w2[2].wait_recv()
    w2[3].wait_recv()
    w3.append(put(wv.at[1, :, block(1)], wv.at[1, :, block(3)], partner))
    finish(0, own4)

    early = len(started)
    sent = list(started)
    whole = [keep(xv, xo0), keep(dv, do0)]
    for copy in w1 + w3:
        copy.wait_recv()

    def forward(ref, m, acts, n):
        rows = acts[pl.ds(n * 2, 2)].reshape(256, 4096)
        ref[:, pl.ds(pl.multiple_of(n * 256, 256), 256)] = dot_nt(wv[m], rows).astype(jnp.bfloat16)

    def pointwise(h, inner, outer):
        @pl.loop(0, 43)
        def _(n):
            rows = pl.ds(pl.multiple_of(n * 16, 16), 16)
            gate = h[0, rows, :].astype(jnp.float32)
            up = h[1, rows, :].astype(jnp.float32)
            sigma = 1.0 / (1.0 + jnp.exp(-gate))
            active = gate * sigma
            if inner:
                h[2, rows, :] = (active * up).astype(jnp.bfloat16)
            if outer:
                back = back_ref[rows, :].astype(jnp.float32)
                h[0, rows, :] = (back * up * sigma * (1.0 + gate * (1.0 - sigma))).astype(jnp.bfloat16)
                h[1, rows, :] = (back * active).astype(jnp.bfloat16)

    for m, acts in enumerate((xv, xv, dv)):
        @pl.loop(0, 2)
        def _(n):
            forward((hv.at[0], hv.at[1], back_ref)[m], m, acts, n)

    far4 = second_axis_far(1, far3)
    pointwise(hv, True, True)
    swap0 = put(hv, hp0, partner)
    rest(1, far3)
    for copy in whole:
        copy.wait()
    for copy in sent:
        copy.wait_send()
    whole = [keep(xo1.at[first], xv.at[first]), keep(xo1.at[2], xv.at[2]), keep(do1.at[:, pl.ds(0, 3)], dv.at[:, pl.ds(0, 3)])]

    @pl.loop(0, 8)
    def _(n):
        span = pl.ds(pl.multiple_of(n * 512, 512), 512)
        total = dot_tn(hv[0], wv[0, :, span]) + dot_tn(hv[1], wv[1, :, span])
        dxv[:, :, :, span] = total.reshape(4, 4, 32, 512)

    def slab(c, k, h):
        span = pl.ds(2048 * c + 1024 * h, 1024)
        return dxv.at[:, k, :, span] if c == 0 else dxv.at[k, :, :, span]

    def part(c, k, h):
        return r2.at[c, h, k]

    ways = ((yleft, yright), (zleft, zright))

    def send_raw(view, way, c, a1, a3):
        return [
            put(view(c, 3, 0), a1.at[c, 0], way[1]),
            put(view(c, 3, 1), a1.at[c, 1], way[0]),
            put(view(c, 2, 1), a3.at[c, 1], way[1]),
            put(view(c, 1, 0), a3.at[c, 0], way[0]),
        ]

    def send_summed(view, way, c, a1, a2, copies):
        copies[0].wait_recv()
        a1[c, 0] += view(c, 2, 0)[...]
        one = put(a1.at[c, 0], a2.at[c, 0], way[1])
        copies[1].wait_recv()
        a1[c, 1] += view(c, 1, 1)[...]
        return [one, put(a1.at[c, 1], a2.at[c, 1], way[0])]

    sums1 = [send_raw(slab, ways[c], c, r1, r3) for c in range(2)]
    whole[0].wait()
    forward(h1.at[0], 0, xv, 0)
    forward(h1.at[1], 1, xv, 0)
    finish(1, far4)
    last_x, last_d = keep(xo1.at[3], xv.at[3]), keep(do1.at[:, 3], dv.at[:, 3])
    whole[1].wait()
    last_x.wait()
    forward(h1.at[0], 0, xv, 1)
    forward(h1.at[1], 1, xv, 1)
    pointwise(h1, True, False)
    swaps = {2: put(h1.at[2], hp1.at[2], partner)}
    for copy in gathered:
        copy.wait_recv()

    def load(k, tokens, theirs, r):
        return [
            keep(source, (xv, dv)[k].at[:, :, :, block(q)])
            for q, source in enumerate((tokens[0].at[:, :, :, block(r)], tokens[1].at[:, :, :, block(r)], theirs.at[0, :, :, :, block(r)], theirs.at[1, :, :, :, block(r)]))
        ]

    loads_x = load(0, (xo0, xo1), xp, 1)
    whole[2].wait()
    last_d.wait()

    @pl.loop(0, 2)
    def _(n):
        forward(back_ref, 2, dv, n)

    loads_d = load(1, (do0, do1), dp, 1)
    pointwise(h1, False, True)
    for m in range(2):
        swaps[m] = put(h1.at[m], hp1.at[m], partner)

    def product(m, acts, n):
        total = None
        for q, h in enumerate((hv, h1, hp0, hp1)):
            span = pl.ds(pl.multiple_of(q * 1024 + n * 256, 256), 256)
            term = jnp.dot(h[m], acts[:, :, :, span].reshape(512, 256), preferred_element_type=jnp.float32)
            total = term if total is None else total + term
        return total

    crossing = {}

    def outgoing(m, acts):
        for half in range(4):
            @pl.loop(half, half + 1)
            def _(n):
                wv[m, :, pl.ds(pl.multiple_of(n * 256, 256), 256)] = product(m, acts, n).astype(jnp.bfloat16)

            span = pl.ds(256 * half, 256)
            crossing[m, half] = [put(wv.at[m, head, span], wr.at[m, head, span], xright), put(wv.at[m, tail, span], wr.at[m, tail, span], xleft)]

    def kept(m, acts, ref):
        @pl.loop(0, 4)
        def _(n):
            ref[:, pl.ds(pl.multiple_of(n * 256, 256), 256)] = product(m, acts, n)

    def close(m, ref):
        for half in range(4):
            for copy in crossing[m, half]:
                copy.wait_recv()

            @pl.loop(half, half + 1)
            def _(n):
                span = pl.ds(pl.multiple_of(n * 256, 256), 256)
                ref[:, span] += wr[m, :, span].astype(jnp.float32)

    for copy in loads_d:
        copy.wait()
    swap0.wait_recv()
    swaps[2].wait_recv()
    outgoing(2, dv)
    loads_d = load(1, (do0, do1), dp, 0)
    sums2 = [send_summed(slab, ways[c], c, r1, r2, sums1[c]) for c in range(2)]
    for copy in loads_x:
        copy.wait()
    swaps[0].wait_recv()
    outgoing(0, xv)
    swaps[1].wait_recv()
    outgoing(1, xv)
    loads_x = load(0, (xo0, xo1), xp, 0)
    for copy in loads_d:
        copy.wait()
    kept(2, dv, od)
    sums3 = []
    for c in range(2):
        sums1[c][3].wait_recv()
        sums2[c][0].wait_recv()
        r2[c, 0] += slab(c, 0, 0)[...] + r3[c, 0]
        sums1[c][2].wait_recv()
        sums2[c][1].wait_recv()
        r2[c, 1] += slab(c, 0, 1)[...] + r3[c, 1]
        sums3.append(send_raw(part, ways[1 - c], c, t1, t3))
    for copy in loads_x:
        copy.wait()
    kept(0, xv, og)
    sums4 = [send_summed(part, ways[1 - c], c, t1, t2, sums3[c]) for c in range(2)]
    kept(1, xv, ou)
    close(2, od)
    for c in range(2):
        sums3[c][3].wait_recv()
        sums4[c][0].wait_recv()
        sums3[c][2].wait_recv()
        sums4[c][1].wait_recv()
        for h in range(2):
            total = part(c, 0, h)[...] + (t2[c, h] + t3[c, h])
            gi[:, pl.ds(pl.multiple_of(owners[2 * c + h] * 1024, 1024), 1024)] = total.astype(jnp.bfloat16)
    close(0, og)
    close(1, ou)
    for copy in started[early:]:
        copy.wait_send()


SENDS, KEPT, LIMIT = 132, 42, 58000000


def body(inputs, w_gate, w_up, w_down, d_out):
    b, f = jnp.bfloat16, jnp.float32
    vm = pl.BlockSpec(memory_space=pltpu.VMEM)
    anys = pl.BlockSpec(memory_space=pl.ANY)
    s = jax.ShapeDtypeStruct
    outs = pl.pallas_call(
        kernel,
        out_shape=[pltpu.VMEM((32, 4096), b)] + [pltpu.VMEM((688, 1024), f)] * 3 + [s((4, 4, 32, 4096), b)] * 4 + [s((2, 4, 4, 32, 2048), b)] * 2,
        in_specs=[anys] * 5,
        out_specs=[vm] * 4 + [anys] * 6,
        scratch_shapes=[pltpu.VMEM((32, 4096), b)] * 4
        + [pltpu.VMEM((3, 688, 4096), b)]
        + [pltpu.VMEM((4, 4, 32, 4096), b)] * 2
        + [pltpu.VMEM((688, 512), b)]
        + [pltpu.VMEM((3, 688, 512), b)] * 4
        + [pltpu.VMEM((4, 4, 32, 4096), f)]
        + [pltpu.VMEM((2, 2, 4, 32, 1024), f)] * 3
        + [pltpu.VMEM((2, 2, 32, 1024), f)] * 3
        + [pltpu.VMEM((3, 688, 1024), b)]
        + [pltpu.SemaphoreType.DMA((SENDS,)), pltpu.SemaphoreType.DMA((SENDS,)), pltpu.SemaphoreType.DMA((KEPT,))],
        compiler_params=pltpu.CompilerParams(collective_id=0, has_side_effects=True, vmem_limit_bytes=LIMIT),
    )(inputs, d_out, w_gate.T, w_up.T, w_down)
    return outs[0], outs[1].T, outs[2].T, outs[3]


def solution(mesh):
    tok = P(("rep", "fs", "tp"), None)
    return jax.shard_map(
        body,
        mesh=mesh,
        in_specs=(tok, P("fs", "tp"), P("fs", "tp"), P("tp", "fs"), tok),
        out_specs=(tok, P("fs", "tp"), P("fs", "tp"), P("tp", "fs")),
        check_vma=False,
    )
```

```python
import jax
import jax.numpy as jnp
from jax import lax
from jax.experimental import pallas as pl
from jax.experimental.pallas import tpu as pltpu
from jax.sharding import PartitionSpec as P

MESH = pl.DeviceIdType.MESH
CUT = 352


def dot_nt(a, b):
    return lax.dot_general(a, b, (((1,), (1,)), ((), ())), preferred_element_type=jnp.float32)


def dot_tn(a, b):
    return lax.dot_general(a, b, (((0,), (0,)), ((), ())), preferred_element_type=jnp.float32)


def kernel(x_ref, d_ref, wg_ref, wu_ref, wd_ref, gi, og, ou, od, xo0, xo1, do0, do1, xp, dp, xs, ds, fx, fd, wv, xv, dv, back_ref, hv, h1, hp0, hp1, dxv, r1, r2, r3, t1, t2, t3, wr, send, recv, local):
    xo, do = (xv, xo1), (dv, do1)
    rep, fs, tp = lax.axis_index("rep"), lax.axis_index("fs"), lax.axis_index("tp")
    core = fs % 2
    xc = rep * 2 + fs // 2
    z, y = tp // 4, tp % 4

    def at_x(v):
        return {"rep": v // 2, "fs": (v % 2) * 2 + core}

    xright, xleft = at_x((xc + 1) % 4), at_x((xc + 3) % 4)
    yright, yleft = {"tp": z * 4 + (y + 1) % 4}, {"tp": z * 4 + (y + 3) % 4}
    zright, zleft = {"tp": ((z + 1) % 4) * 4 + y}, {"tp": ((z + 3) % 4) * 4 + y}
    partner = {"fs": fs + 1 - 2 * core}
    owners = (fs, (fs + 2) % 4, fs + 1 - 2 * core, 3 - fs)
    counts = [0]

    def keep(src, dst):
        copy = pltpu.make_async_copy(src, dst, local.at[counts[0]])
        counts[0] += 1
        copy.start()
        return copy

    started = []

    def put(src, dst, dev):
        n = len(started)
        copy = pltpu.make_async_remote_copy(src_ref=src, dst_ref=dst, send_sem=send.at[n], recv_sem=recv.at[n], device_id=dev, device_id_type=MESH)
        copy.start()
        started.append(copy)
        return copy

    def block(r):
        return pl.ds(1024 * r, 1024)

    ready = []
    for q, owner in enumerate(owners):
        span = pl.ds(pl.multiple_of(owner * 1024, 1024), 1024)
        ready += [keep(x_ref.at[:, span], xs.at[:, block(q)]), keep(d_ref.at[:, span], ds.at[:, block(q)])]
    for m, ref in enumerate((wg_ref, wu_ref, wd_ref)):
        ready.append(keep(ref, wv.at[m, :, block(0)]))

    barrier = pltpu.get_barrier_semaphore()
    for dev in (xright, xleft, yright, yleft, zright, zleft, partner):
        pl.semaphore_signal(barrier, inc=1, device_id=dev, device_id_type=MESH)
    pl.semaphore_wait(barrier, 7)
    for copy in ready[:8]:
        copy.wait()

    head, tail = pl.ds(0, CUT), pl.ds(CUT, 688 - CUT)
    lo, hi = pl.ds(0, 16), pl.ds(16, 16)
    first, second = pl.ds(0, 2), pl.ds(2, 2)
    gathered = []

    def first_axis(k, xsrc, dsrc):
        return [
            put(xsrc, xo[k].at[0, 1], yright),
            put(dsrc, do[k].at[1, 0], zright),
            put(xsrc, xo[k].at[0, 2], yleft),
            put(dsrc, do[k].at[2, 0], zleft),
        ]

    def first_axis_far(k, c):
        c[0].wait_recv()
        a = put(xo[k].at[0, 1, lo], xo[k].at[0, 3, lo], yright)
        c[1].wait_recv()
        b = put(do[k].at[1, 0, lo], do[k].at[3, 0, lo], zright)
        c[2].wait_recv()
        e = put(xo[k].at[0, 2, hi], xo[k].at[0, 3, hi], yleft)
        c[3].wait_recv()
        f = put(do[k].at[2, 0, hi], do[k].at[3, 0, hi], zleft)
        return [a, e, b, f]

    def hand_x(k, a):
        gathered.append(put(xo[k].at[a, :, :, pl.ds(2048, 2048)], xp.at[k, a], partner))

    def hand_d(k, a):
        gathered.append(put(do[k].at[:, a, :, pl.ds(2048, 2048)], dp.at[k, :, a], partner))

    def second_axis(k, c):
        c[0].wait_recv()
        c[1].wait_recv()
        x = [put(xo[k].at[0, half], xo[k].at[slot, half], dev) for half, slot, dev in ((first, 1, zright), (second, 2, zleft), (second, 1, zright), (first, 2, zleft))]
        c[2].wait_recv()
        c[3].wait_recv()
        d = [put(do[k].at[half, 0], do[k].at[half, slot], dev) for half, slot, dev in ((first, 1, yright), (second, 2, yleft), (second, 1, yright), (first, 2, yleft))]
        hand_x(k, 0)
        hand_d(k, 0)
        return x, d

    def second_axis_far(k, c):
        first, second = ((pl.ds(0, 2), pl.ds(2, 2)), (pl.ds(0, 2), pl.ds(2, 2)))[k]
        x, d = c
        x[0].wait_recv()
        a = put(xo[k].at[1, first], xo[k].at[3, first], zright)
        d[0].wait_recv()
        b = put(do[k].at[first, 1], do[k].at[first, 3], yright)
        x[1].wait_recv()
        e = put(xo[k].at[2, second], xo[k].at[3, second], zleft)
        d[1].wait_recv()
        f = put(do[k].at[second, 2], do[k].at[second, 3], yleft)
        return [a, e, b, f]

    def rest(k, c):
        x, d = c
        for n in range(2):
            x[2 + n].wait_recv()
            hand_x(k, 1 + n)
            d[2 + n].wait_recv()
            hand_d(k, 1 + n)

    def finish(k, c):
        c[0].wait_recv()
        c[1].wait_recv()
        hand_x(k, 3)
        c[2].wait_recv()
        c[3].wait_recv()
        hand_d(k, 3)

    hops = [put(xs, fx, xright), put(ds, fd, xleft)]
    own1 = first_axis(0, xs, ds)
    own0 = [keep(xs, xo[0].at[0, 0]), keep(ds, do[0].at[0, 0])]

    for copy in ready[8:]:
        copy.wait()
    w1 = [put(wv.at[m, :, block(0)], wv.at[m, :, block(2)], partner) for m in range(3)]
    hops[0].wait_recv()
    far = [put(fx, xo[1].at[0, 0], xright)]
    hops[1].wait_recv()
    far.append(put(fd, do[1].at[0, 0], xleft))
    w2 = [
        put(wv.at[0, :, block(0)], wv.at[0, :, block(1)], xright),
        put(wv.at[2, :, block(0)], wv.at[2, :, block(1)], xleft),
        put(wv.at[1, head, block(0)], wv.at[1, head, block(1)], xright),
        put(wv.at[1, tail, block(0)], wv.at[1, tail, block(1)], xleft),
    ]
    own2 = first_axis_far(0, own1)
    for copy in own0:
        copy.wait()
    own3 = second_axis(0, own2)
    far[0].wait_recv()
    far[1].wait_recv()
    far1 = first_axis(1, xo[1].at[0, 0], do[1].at[0, 0])
    far2 = first_axis_far(1, far1)
    own4 = second_axis_far(0, own3)
    w2[0].wait_recv()
    w3 = [put(wv.at[0, :, block(1)], wv.at[0, :, block(3)], partner)]
    w2[1].wait_recv()
    w3.append(put(wv.at[2, :, block(1)], wv.at[2, :, block(3)], partner))
    rest(0, own3)
    far3 = second_axis(1, far2)
    w2[2].wait_recv()
    w2[3].wait_recv()
    w3.append(put(wv.at[1, :, block(1)], wv.at[1, :, block(3)], partner))
    finish(0, own4)

    early = len(started)
    sent = list(started)
    whole = [keep(xv, xo0), keep(dv, do0)]
    for copy in w1 + w3:
        copy.wait_recv()

    def forward(ref, m, acts, n):
        rows = acts[pl.ds(n * 2, 2)].reshape(256, 4096)
        ref[:, pl.ds(pl.multiple_of(n * 256, 256), 256)] = dot_nt(wv[m], rows).astype(jnp.bfloat16)

    def pointwise(h, inner, outer):
        @pl.loop(0, 43)
        def _(n):
            rows = pl.ds(pl.multiple_of(n * 16, 16), 16)
            gate = h[0, rows, :].astype(jnp.float32)
            up = h[1, rows, :].astype(jnp.float32)
            sigma = 1.0 / (1.0 + jnp.exp(-gate))
            active = gate * sigma
            if inner:
                h[2, rows, :] = (active * up).astype(jnp.bfloat16)
            if outer:
                back = back_ref[rows, :].astype(jnp.float32)
                h[0, rows, :] = (back * up * sigma * (1.0 + gate * (1.0 - sigma))).astype(jnp.bfloat16)
                h[1, rows, :] = (back * active).astype(jnp.bfloat16)

    for m, acts in enumerate((xv, xv, dv)):
        @pl.loop(0, 2)
        def _(n):
            forward((hv.at[0], hv.at[1], back_ref)[m], m, acts, n)

    far4 = second_axis_far(1, far3)
    pointwise(hv, True, True)
    swap0 = put(hv, hp0, partner)
    rest(1, far3)
    for copy in whole:
        copy.wait()
    for copy in sent:
        copy.wait_send()
    whole = [keep(xo1.at[first], xv.at[first]), keep(xo1.at[2], xv.at[2]), keep(do1.at[:, pl.ds(0, 3)], dv.at[:, pl.ds(0, 3)])]

    @pl.loop(0, 8)
    def _(n):
        span = pl.ds(pl.multiple_of(n * 512, 512), 512)
        total = dot_tn(hv[0], wv[0, :, span]) + dot_tn(hv[1], wv[1, :, span])
        dxv[:, :, :, span] = total.reshape(4, 4, 32, 512)

    def slab(c, k, h):
        span = pl.ds(2048 * c + 1024 * h, 1024)
        return dxv.at[:, k, :, span] if c == 0 else dxv.at[k, :, :, span]

    def part(c, k, h):
        return r2.at[c, h, k]

    ways = ((yleft, yright), (zleft, zright))

    def send_raw(view, way, c, a1, a3):
        return [
            put(view(c, 3, 0), a1.at[c, 0], way[1]),
            put(view(c, 3, 1), a1.at[c, 1], way[0]),
            put(view(c, 2, 1), a3.at[c, 1], way[1]),
            put(view(c, 1, 0), a3.at[c, 0], way[0]),
        ]

    def send_summed(view, way, c, a1, a2, copies):
        copies[0].wait_recv()
        a1[c, 0] += view(c, 2, 0)[...]
        one = put(a1.at[c, 0], a2.at[c, 0], way[1])
        copies[1].wait_recv()
        a1[c, 1] += view(c, 1, 1)[...]
        return [one, put(a1.at[c, 1], a2.at[c, 1], way[0])]

    sums1 = [send_raw(slab, ways[c], c, r1, r3) for c in range(2)]
    whole[0].wait()
    forward(h1.at[0], 0, xv, 0)
    forward(h1.at[1], 1, xv, 0)
    finish(1, far4)
    last_x, last_d = keep(xo1.at[3], xv.at[3]), keep(do1.at[:, 3], dv.at[:, 3])
    whole[1].wait()
    last_x.wait()
    forward(h1.at[0], 0, xv, 1)
    forward(h1.at[1], 1, xv, 1)
    pointwise(h1, True, False)
    swaps = {2: put(h1.at[2], hp1.at[2], partner)}

    def load(k, tokens, theirs, r):
        return [
            keep(source, (xv, dv)[k].at[:, :, :, block(q)])
            for q, source in enumerate((tokens[0].at[:, :, :, block(r)], tokens[1].at[:, :, :, block(r)], theirs.at[0, :, :, :, block(r)], theirs.at[1, :, :, :, block(r)]))
        ]

    whole[2].wait()
    last_d.wait()

    @pl.loop(0, 2)
    def _(n):
        forward(back_ref, 2, dv, n)

    for copy in gathered:
        copy.wait_recv()
    loads_d = load(1, (do0, do1), dp, 1)
    loads_x = load(0, (xo0, xo1), xp, 1)
    pointwise(h1, False, True)
    for m in range(2):
        swaps[m] = put(h1.at[m], hp1.at[m], partner)

    def product(m, acts, n):
        total = None
        for q, h in enumerate((hv, h1, hp0, hp1)):
            span = pl.ds(pl.multiple_of(q * 1024 + n * 256, 256), 256)
            term = jnp.dot(h[m], acts[:, :, :, span].reshape(512, 256), preferred_element_type=jnp.float32)
            total = term if total is None else total + term
        return total

    crossing = {}

    def outgoing(m, acts):
        for half in range(4):
            @pl.loop(half, half + 1)
            def _(n):
                wv[m, :, pl.ds(pl.multiple_of(n * 256, 256), 256)] = product(m, acts, n).astype(jnp.bfloat16)

            span = pl.ds(256 * half, 256)
            crossing[m, half] = [put(wv.at[m, head, span], wr.at[m, head, span], xright), put(wv.at[m, tail, span], wr.at[m, tail, span], xleft)]

    def kept(m, acts, ref):
        @pl.loop(0, 4)
        def _(n):
            ref[:, pl.ds(pl.multiple_of(n * 256, 256), 256)] = product(m, acts, n)

    def close(m, ref):
        for half in range(4):
            for copy in crossing[m, half]:
                copy.wait_recv()

            @pl.loop(half, half + 1)
            def _(n):
                span = pl.ds(pl.multiple_of(n * 256, 256), 256)
                ref[:, span] += wr[m, :, span].astype(jnp.float32)

    for copy in loads_d:
        copy.wait()
    swap0.wait_recv()
    swaps[2].wait_recv()
    outgoing(2, dv)
    loads_d = load(1, (do0, do1), dp, 0)
    sums2 = [send_summed(slab, ways[c], c, r1, r2, sums1[c]) for c in range(2)]
    for copy in loads_x:
        copy.wait()
    swaps[0].wait_recv()
    outgoing(0, xv)
    swaps[1].wait_recv()
    outgoing(1, xv)
    loads_x = load(0, (xo0, xo1), xp, 0)
    for copy in loads_d:
        copy.wait()
    kept(2, dv, od)
    sums3 = []
    for c in range(2):
        sums1[c][3].wait_recv()
        sums2[c][0].wait_recv()
        r2[c, 0] += slab(c, 0, 0)[...] + r3[c, 0]
        sums1[c][2].wait_recv()
        sums2[c][1].wait_recv()
        r2[c, 1] += slab(c, 0, 1)[...] + r3[c, 1]
        sums3.append(send_raw(part, ways[1 - c], c, t1, t3))
    for copy in loads_x:
        copy.wait()
    kept(0, xv, og)
    sums4 = [send_summed(part, ways[1 - c], c, t1, t2, sums3[c]) for c in range(2)]
    kept(1, xv, ou)
    close(2, od)
    for c in range(2):
        sums3[c][3].wait_recv()
        sums4[c][0].wait_recv()
        sums3[c][2].wait_recv()
        sums4[c][1].wait_recv()
        for h in range(2):
            total = part(c, 0, h)[...] + (t2[c, h] + t3[c, h])
            gi[:, pl.ds(pl.multiple_of(owners[2 * c + h] * 1024, 1024), 1024)] = total.astype(jnp.bfloat16)
    close(0, og)
    close(1, ou)
    for copy in started[early:]:
        copy.wait_send()


SENDS, KEPT, LIMIT = 132, 42, 58000000


def body(inputs, w_gate, w_up, w_down, d_out):
    b, f = jnp.bfloat16, jnp.float32
    vm = pl.BlockSpec(memory_space=pltpu.VMEM)
    anys = pl.BlockSpec(memory_space=pl.ANY)
    s = jax.ShapeDtypeStruct
    outs = pl.pallas_call(
        kernel,
        out_shape=[pltpu.VMEM((32, 4096), b)] + [pltpu.VMEM((688, 1024), f)] * 3 + [s((4, 4, 32, 4096), b)] * 4 + [s((2, 4, 4, 32, 2048), b)] * 2,
        in_specs=[anys] * 5,
        out_specs=[vm] * 4 + [anys] * 6,
        scratch_shapes=[pltpu.VMEM((32, 4096), b)] * 4
        + [pltpu.VMEM((3, 688, 4096), b)]
        + [pltpu.VMEM((4, 4, 32, 4096), b)] * 2
        + [pltpu.VMEM((688, 512), b)]
        + [pltpu.VMEM((3, 688, 512), b)] * 4
        + [pltpu.VMEM((4, 4, 32, 4096), f)]
        + [pltpu.VMEM((2, 2, 4, 32, 1024), f)] * 3
        + [pltpu.VMEM((2, 2, 32, 1024), f)] * 3
        + [pltpu.VMEM((3, 688, 1024), b)]
        + [pltpu.SemaphoreType.DMA((SENDS,)), pltpu.SemaphoreType.DMA((SENDS,)), pltpu.SemaphoreType.DMA((KEPT,))],
        compiler_params=pltpu.CompilerParams(collective_id=0, has_side_effects=True, vmem_limit_bytes=LIMIT),
    )(inputs, d_out, w_gate.T, w_up.T, w_down)
    return outs[0], outs[1].T, outs[2].T, outs[3]


def solution(mesh):
    tok = P(("rep", "fs", "tp"), None)
    return jax.shard_map(
        body,
        mesh=mesh,
        in_specs=(tok, P("fs", "tp"), P("fs", "tp"), P("tp", "fs"), tok),
        out_specs=(tok, P("fs", "tp"), P("fs", "tp"), P("tp", "fs")),
        check_vma=False,
    )
```
